256 devices in a mesh: sp: 64 (over z, x, core), tp: 4 (over y).
Axes of the slice: x: 4, y: 4, z: 8, core: 2. Of those that a mesh axis runs over, the one named last changes fastest.
Arguments:
- residual: bfloat16 [32768, 2048], P(('sp', 'tp')), may hold values from -6 to 6
- queries: bfloat16 [32768, 1024], P('sp', 'tp'), may hold values from -6 to 6
- key_vectors: bfloat16 [32768, 1024], P('sp', 'tp'), may hold values from -6 to 6
- value_vectors: bfloat16 [32768, 1024], P('sp', 'tp'), may hold values from -6 to 6
- output_gate: bfloat16 [32768, 1024], P('sp', 'tp'), may hold values from -6 to 6
- input_gate: float32 [32768, 16], P('sp', 'tp'), may hold values from -4 to 250
- forget_gate: float32 [32768, 16], P('sp', 'tp'), may hold values from 0 to 20
- head_gain: float32 [16, 64], P('tp'), may hold values from 0.1 to 1.9
- output_weight: bfloat16 [1024, 2048], replicated, may hold values from -0.1875 to 0.1875
- norm_gain: float32 [2048], replicated, may hold values from 0.1 to 1.9
- route_experts: int32 [32768, 2], P('sp'), may hold values from 0 to 63, as said below
- group_weight: float32 [32768], P('sp'), may hold values from 0.25 to 1
- expert_scores: float32 [32768, 2], P('sp'), may hold values from -6 to 6
- gate_weight: bfloat16 [64, 2048, 1024], P('sp', None, 'tp'), may hold values from -0.125 to 0.125
- up_weight: bfloat16 [64, 2048, 1024], P('sp', None, 'tp'), may hold values from -0.125 to 0.125
- down_weight: bfloat16 [64, 1024, 2048], P('sp', 'tp'), may hold values from -0.1875 to 0.1875
Outputs:
- mixed_out: bfloat16 [32768, 2048], P(('sp', 'tp'))
The draws below stay inside these ranges and needn't reach their ends.
Inputs may be any that keep to these rules, and one draw needn't show every extreme that they name: `route_experts`: the two experts of a row differ and lie in the same group of 16 consecutive experts. In each aligned block of 128 rows no expert is named more than 8 times, and in every block some expert is named exactly 8 times.
All inputs are finite; a program needn't handle non-finite values.
Results may differ from the reference program's by a relative error of at most 0.012.
Values may be sent and summed in bfloat16 or wider, within the bound.
A program may use at most 128 MiB of HBM per device.

```python
import jax
import jax.numpy as jnp
from jax import lax

D = 2048
CELL_HEAD_COUNT = 16
HEAD = 64
MIX = 1024
FFE = 1024
GROUPS = 4
TOP = 2
BLOCK = 128
TOK_DEV = 128
SEQUENCE_TOKENS = 32768
EXPERTS = 64
CAP = 8
N_TP = 4


def draw_input_gate(key, part):
    base_value = jnp.clip(jax.random.normal(jax.random.fold_in(key, 11), (SEQUENCE_TOKENS, CELL_HEAD_COUNT), jnp.float32), -4.0, 4.0)
    return base_value


def draw_forget_gate(key, part):
    head_order = jax.random.permutation(jax.random.fold_in(key, 21), CELL_HEAD_COUNT)
    slow_count = CELL_HEAD_COUNT // 2
    sluggish_heads = head_order < slow_count
    step_rate = jnp.where(sluggish_heads, 0.6 / SEQUENCE_TOKENS, 1.0 / 40.0).astype(jnp.float32)
    device_span = SEQUENCE_TOKENS // EXPERTS
    factor = jnp.exp(jax.random.uniform(jax.random.fold_in(key, 22), (SEQUENCE_TOKENS // device_span, CELL_HEAD_COUNT), jnp.float32, -0.6931, 0.6931))
    factor = jnp.repeat(factor, device_span, axis=0)
    jitter = jnp.clip(0.7 * jax.random.normal(jax.random.fold_in(key, 23), (SEQUENCE_TOKENS, CELL_HEAD_COUNT), jnp.float32), -2.1, 2.1)
    gate_preactivation = -jnp.log(step_rate[None, :] * factor) + jitter
    surge_mask = (jax.random.uniform(jax.random.fold_in(key, 24), (SEQUENCE_TOKENS, CELL_HEAD_COUNT), jnp.float32) < 1.5 / SEQUENCE_TOKENS) & sluggish_heads[None, :]
    retained_fraction = 0.6 + 0.2 * jax.random.uniform(jax.random.fold_in(key, 25), (SEQUENCE_TOKENS, CELL_HEAD_COUNT), jnp.float32)
    return jnp.where(surge_mask, jnp.log(retained_fraction / (1.0 - retained_fraction)), gate_preactivation)


def draw_route_experts(key, part):
    block_total = SEQUENCE_TOKENS // TOK_DEV
    per_group = EXPERTS // GROUPS
    places = EXPERTS * CAP // 2
    position = jnp.arange(places, dtype=jnp.int32)
    group_of = position // (per_group * CAP // 2)
    inner_index = position % (per_group * CAP // 2)
    round_index = inner_index // per_group
    first_slot = inner_index % per_group
    second = (first_slot + 1 + round_index % (per_group - 1)) % per_group
    hot_expert = jax.random.randint(jax.random.fold_in(key, 31), (), 0, EXPERTS, dtype=jnp.int32)
    involved = (group_of == hot_expert // per_group) & ((first_slot == hot_expert % per_group) | (second == hot_expert % per_group))

    def one_block(block_key):
        rank_order = jax.random.permutation(jax.random.fold_in(block_key, 1), places).astype(jnp.int32)
        priority = rank_order + places * involved.astype(jnp.int32)
        _, chosen = lax.top_k(priority, TOK_DEV)
        chosen = chosen[jax.random.permutation(jax.random.fold_in(block_key, 2), TOK_DEV)]
        swap_order = jax.random.randint(jax.random.fold_in(block_key, 3), (TOK_DEV,), 0, 2, dtype=jnp.int32)
        expert_first = group_of[chosen] * per_group + first_slot[chosen]
        expert_second = group_of[chosen] * per_group + second[chosen]
        left_side = jnp.where(swap_order == 1, expert_second, expert_first)
        right_side = jnp.where(swap_order == 1, expert_first, expert_second)
        return jnp.stack([left_side, right_side], axis=1)
    block_keys = jax.random.split(jax.random.fold_in(key, 32), block_total)
    return jax.vmap(one_block)(block_keys).reshape(SEQUENCE_TOKENS, TOP).astype(jnp.int32)


def steps_of(key, extent, cuts, low, high):
    factor_of = 1.0
    for dim, blocks in cuts:
        steps = jax.random.uniform(jax.random.fold_in(jax.random.fold_in(key, 6), dim), (blocks,), jnp.float32, low / len(cuts), high / len(cuts))
        factor_of = factor_of * jnp.repeat(jnp.exp(steps), extent[dim] // blocks).reshape((-1,) + (1,) * (len(extent) - 1 - dim))
    return factor_of


def gaussian(rng, shape, width, bound, cuts=(), held_as=jnp.bfloat16):
    array = width * jax.random.normal(rng, shape, jnp.float32)
    if cuts:
        array = array * steps_of(rng, shape, cuts, -0.22, 0.18)
    return jnp.clip(array, -bound, bound).astype(held_as)


def setup_inputs(seed: int = 0) -> dict:
    streams_of = jax.random.split(jax.random.key(seed), 17)
    residual = gaussian(streams_of[0], (SEQUENCE_TOKENS, D), 1.0, 6.0, ((0, 256),))
    queries = gaussian(streams_of[1], (SEQUENCE_TOKENS, MIX), 1.0, 6.0, ((0, 64), (1, 4)))
    key_vectors = gaussian(streams_of[2], (SEQUENCE_TOKENS, MIX), 1.0, 6.0, ((0, 64), (1, 4)))
    value_vectors = gaussian(streams_of[3], (SEQUENCE_TOKENS, MIX), 1.0, 6.0, ((0, 64), (1, 4)))
    output_gate = gaussian(streams_of[4], (SEQUENCE_TOKENS, MIX), 1.0, 6.0, ((0, 64), (1, 4)))
    input_gate = draw_input_gate(jax.random.fold_in(streams_of[16], 71), 0)
    forget_gate = draw_forget_gate(jax.random.fold_in(streams_of[16], 71), 0)
    head_gain = jnp.clip(1.0 + 0.18 * jax.random.normal(streams_of[7], (CELL_HEAD_COUNT, HEAD), jnp.float32), 0.1, 1.9)
    output_weight = gaussian(streams_of[8], (MIX, D), MIX ** -0.5, 0.1875)
    norm_gain = jnp.clip(1.0 + 0.18 * jax.random.normal(streams_of[9], (D,), jnp.float32), 0.1, 1.9)
    route_experts = draw_route_experts(jax.random.fold_in(streams_of[16], 71), 0)
    group_weight = jnp.clip(0.25 + 0.75 * jax.random.uniform(streams_of[11], (SEQUENCE_TOKENS,), jnp.float32) ** steps_of(streams_of[11], (SEQUENCE_TOKENS,), ((0, 64),), -0.2, 0.2), 0.25, 1.0)
    expert_scores = gaussian(streams_of[12], (SEQUENCE_TOKENS, TOP), 1.5, 6.0, ((0, 64),), jnp.float32)
    gate_weight = gaussian(streams_of[13], (EXPERTS, D, FFE), D ** -0.5, 0.125, ((0, 64), (2, 4)))
    up_weight = gaussian(streams_of[14], (EXPERTS, D, FFE), D ** -0.5, 0.125, ((0, 64), (2, 4)))
    down_weight = gaussian(streams_of[15], (EXPERTS, FFE, D), FFE ** -0.5, 0.1875, ((0, 64), (1, 4)))
    return {"residual": residual, "queries": queries, "key_vectors": key_vectors, "value_vectors": value_vectors, "output_gate": output_gate, "input_gate": input_gate, "forget_gate": forget_gate, "head_gain": head_gain, "output_weight": output_weight, "norm_gain": norm_gain, "route_experts": route_experts, "group_weight": group_weight, "expert_scores": expert_scores, "gate_weight": gate_weight, "up_weight": up_weight, "down_weight": down_weight}


EPSILON = 1e-06
PRECISE = lax.Precision.HIGHEST

def block_step(carried, pieces):
    memory, stabilizer = carried
    query_block, key_block, value_block, decay_block, gate_block = pieces
    block_size = query_block.shape[0]
    causal_mask = jnp.tril(jnp.ones((block_size, block_size), dtype=bool))
    decay_rows = decay_block.T
    gate_rows = gate_block.T
    pair_log = decay_rows[:, :, None] - decay_rows[:, None, :] + gate_rows[:, None, :]
    pair_log = jnp.where(causal_mask[None], pair_log, -jnp.inf)
    carry_log = decay_rows + stabilizer[:, None]
    peak_level = jnp.maximum(carry_log, lax.optimization_barrier(jnp.max(pair_log, axis=-1)))
    within_weight = jnp.exp(pair_log - peak_level[:, :, None])
    carry_weight = jnp.exp(carry_log - peak_level)
    scores = jnp.einsum('thd,shd->hts', query_block, key_block, precision=PRECISE) * within_weight
    numerator = jnp.einsum('hts,shd->htd', scores, value_block, precision=PRECISE)
    numerator = numerator + carry_weight[:, :, None] * jnp.einsum('thd,hde->hte', query_block, memory, precision=PRECISE)
    outputs = jnp.transpose(numerator, (1, 0, 2))
    final_decay = decay_rows[:, -1]
    key_log = final_decay[:, None] - decay_rows + gate_rows
    new_level = jnp.maximum(final_decay + stabilizer, lax.optimization_barrier(jnp.max(key_log, axis=-1)))
    key_weight = jnp.exp(key_log - new_level[:, None])
    carry_fade = jnp.exp(final_decay + stabilizer - new_level)
    memory = carry_fade[:, None, None] * memory + jnp.einsum('hs,shd,she->hde', key_weight, key_block, value_block, precision=PRECISE)
    return ((memory, new_level), outputs)

def cell_outputs(query_part, key_part, value_part, input_gate, log_forget, initial):
    length, head_count, head_size = query_part.shape
    block_count = length // BLOCK
    cumulative = jnp.cumsum(log_forget.reshape(block_count, BLOCK, head_count), axis=1)
    shaped = (query_part.reshape(block_count, BLOCK, head_count, head_size), key_part.reshape(block_count, BLOCK, head_count, head_size), value_part.reshape(block_count, BLOCK, head_count, head_size), cumulative, input_gate.reshape(block_count, BLOCK, head_count))
    _, outputs = lax.scan(block_step, initial, shaped)
    return outputs.reshape(length, head_count, head_size)

def expert_sum(normed, route_experts, route_weight, gate_weight, up_weight, down_weight):
    flat_routes = route_experts.reshape(-1)
    flat_weights = jnp.concatenate([route_weight.reshape(-1), jnp.zeros((1,), jnp.float32)])
    padded = jnp.concatenate([normed, jnp.zeros((1, D), jnp.bfloat16)], axis=0)
    most_rows = CAP * (SEQUENCE_TOKENS // TOK_DEV)
    part_width = FFE // N_TP

    def one_expert(accumulated, expert):
        picked = jnp.nonzero(flat_routes == expert, size=most_rows, fill_value=flat_routes.shape[0])[0]
        token_of = picked // TOP
        chosen_rows = padded[token_of]
        gate_value = jnp.dot(chosen_rows, gate_weight[expert], preferred_element_type=jnp.float32)
        up_value = jnp.dot(chosen_rows, up_weight[expert], preferred_element_type=jnp.float32)
        hidden = (jax.nn.silu(gate_value) * up_value).astype(jnp.bfloat16)
        down_rows = down_weight[expert]
        summed = jnp.zeros((most_rows, D), jnp.float32)
        for quarter in range(N_TP):
            piece_out = jnp.dot(hidden[:, quarter * part_width:(quarter + 1) * part_width], down_rows[quarter * part_width:(quarter + 1) * part_width], preferred_element_type=jnp.float32).astype(jnp.bfloat16)
            summed = summed + lax.optimization_barrier(piece_out).astype(jnp.float32)
        rounded = lax.optimization_barrier(summed.astype(jnp.bfloat16))
        result = rounded.astype(jnp.float32) * flat_weights[picked][:, None]
        return (accumulated.at[token_of].add(result), None)
    accumulated = jnp.zeros((SEQUENCE_TOKENS + 1, D), jnp.float32)
    accumulated, _ = lax.scan(one_expert, accumulated, jnp.arange(EXPERTS, dtype=jnp.int32))
    return accumulated[:SEQUENCE_TOKENS]

def reference(residual, queries, key_vectors, value_vectors, output_gate, input_gate, forget_gate, head_gain, output_weight, norm_gain, route_experts, group_weight, expert_scores, gate_weight, up_weight, down_weight):
    query_part = queries.astype(jnp.float32).reshape(SEQUENCE_TOKENS, CELL_HEAD_COUNT, HEAD) * HEAD ** (-0.5)
    key_part = key_vectors.astype(jnp.float32).reshape(SEQUENCE_TOKENS, CELL_HEAD_COUNT, HEAD)
    value_part = value_vectors.astype(jnp.float32).reshape(SEQUENCE_TOKENS, CELL_HEAD_COUNT, HEAD)
    log_forget = jax.nn.log_sigmoid(forget_gate)
    initial = (jnp.zeros((CELL_HEAD_COUNT, HEAD, HEAD), jnp.float32), jnp.zeros((CELL_HEAD_COUNT,), jnp.float32))
    cell_out = cell_outputs(query_part, key_part, value_part, input_gate, log_forget, initial)
    normed_heads = cell_out * lax.rsqrt(lax.optimization_barrier(jnp.mean(cell_out * cell_out, axis=-1, keepdims=True)) + EPSILON) * head_gain
    mixed_rows = (jax.nn.sigmoid(output_gate.astype(jnp.float32)) * normed_heads.reshape(SEQUENCE_TOKENS, MIX)).astype(jnp.bfloat16)
    projected = jnp.dot(mixed_rows, output_weight, preferred_element_type=jnp.float32)
    stream = (residual.astype(jnp.float32) + projected).astype(jnp.bfloat16)
    stream_float = stream.astype(jnp.float32)
    normed = (stream_float * lax.rsqrt(lax.optimization_barrier(jnp.mean(stream_float * stream_float, axis=-1, keepdims=True)) + EPSILON) * norm_gain).astype(jnp.bfloat16)
    route_weight = group_weight[:, None] * jax.nn.softmax(expert_scores, axis=-1)
    expert_mix = expert_sum(normed, route_experts, route_weight, gate_weight, up_weight, down_weight)
    return (stream_float + expert_mix).astype(jnp.bfloat16)
```

```python
import functools

import jax
import jax.numpy as jnp
from jax import lax
from jax.experimental import pallas as pl
from jax.experimental.pallas import tpu as pltpu
from jax.sharding import PartitionSpec as P

EPSILON = 1e-06
VERY_NEGATIVE = -1e30
MESH = pl.DeviceIdType.MESH
PLANE = 8
F32 = jnp.float32
BF16 = jnp.bfloat16


def dot(a, b):
    return jnp.dot(a, b, preferred_element_type=F32)


def dot_t(a, b):
    return lax.dot_general(a, b, (((1,), (1,)), ((), ())), preferred_element_type=F32)


def halves(x):
    high = x.astype(BF16)
    return high, (x - high.astype(F32)).astype(BF16)


def shifted(x, by, fill):
    lane = lax.broadcasted_iota(jnp.int32, x.shape, 1)
    return jnp.where(lane >= by, pltpu.roll(x, by, 1), fill)


def running(x, combine, fill):
    by = 1
    while by < x.shape[1]:
        x = combine(x, shifted(x, by, fill))
        by *= 2
    return x


def join(early, late):
    early_total, early_level, early_memory = early
    late_total, late_level, late_memory = late
    level = jnp.maximum(late_total + early_level, late_level)
    memory = (
        jnp.exp(late_total + early_level - level) * early_memory
        + jnp.exp(late_level - level) * late_memory
    )
    return early_total + late_total, level, memory


def packed(total, level, memory):
    row = lax.broadcasted_iota(jnp.int32, memory.shape, 0)
    return memory, jnp.where(row == 0, total, jnp.where(row == 1, level, 0.0))


def unpacked(ref, index):
    return ref[index, 8:9, :], ref[index, 9:10, :], ref[index, 0:8, :]


def put(ref, index, state):
    memory, scalars = packed(*state)
    ref[index, 0:8, :] = memory
    ref[index, 8:16, :] = scalars


def ring_peer(me, step, count):
    away = (step + 1) // 2
    sign = 2 * lax.rem(step, 2) - 1
    return lax.rem(me + sign * away + count, count)


def slots_of(routes, capacity, experts):
    tokens = routes.shape[1]
    expert = lax.broadcasted_iota(jnp.int32, (experts, tokens), 0)
    first = expert == routes[0:1, :]
    second = expert == routes[1:2, :]
    row = lax.broadcasted_iota(jnp.int32, (tokens, tokens), 0)
    column = lax.broadcasted_iota(jnp.int32, (tokens, tokens), 1)
    earlier = jnp.where(row < column, 1.0, 0.0).astype(BF16)
    ones = jnp.ones((tokens, tokens), BF16)
    first_hot = jnp.where(first, 1.0, 0.0).astype(BF16)
    second_hot = jnp.where(second, 1.0, 0.0).astype(BF16)
    first_rank = dot(first_hot, earlier)
    second_rank = dot(first_hot, ones) + dot(second_hot, earlier)
    places = []
    for hot, rank, route in ((first, first_rank, routes[0:1, :]), (second, second_rank, routes[1:2, :])):
        own = jnp.sum(jnp.where(hot, rank, 0.0), axis=0, keepdims=True)
        places.append(route * capacity + own.astype(jnp.int32))
    return places


def front_kernel(
    sp_count,
    tp_count,
    head_count,
    q_ref,
    k_ref,
    v_ref,
    og_ref,
    ig_ref,
    fg_ref,
    hgain_ref,
    wo_hbm,
    res_ref,
    ngain_ref,
    routes_ref,
    arrived_ref,
    stream_ref,
    wo_ref,
    intra_ref,
    s1_ref,
    r1_ref,
    s2_ref,
    r2_ref,
    s3_ref,
    r3_ref,
    mix_ref,
    mrecv_ref,
    send_ref,
    wo_sem,
    own_sem,
    send1,
    recv1,
    send2,
    recv2,
    send3,
    recv3,
    send4,
    recv4,
    send5,
    recv5,
):
    me = lax.axis_index("sp")
    mt = lax.axis_index("tp")
    zed = me // PLANE
    place = lax.rem(me, PLANE)
    planes = sp_count // PLANE
    length, width = q_ref.shape
    head = width // head_count
    tokens = length // tp_count

    barrier = pltpu.get_barrier_semaphore()

    def greet(step, _):
        pl.semaphore_signal(
            barrier, inc=1, device_id={"sp": ring_peer(me, step, sp_count)}, device_id_type=MESH
        )
        return 0

    lax.fori_loop(1, sp_count, greet, 0)

    def greet_tp(step, _):
        pl.semaphore_signal(
            barrier, inc=1, device_id={"tp": lax.rem(mt + step, tp_count)}, device_id_type=MESH
        )
        return 0

    lax.fori_loop(1, tp_count, greet_tp, 0)

    wo_copy = pltpu.make_async_copy(wo_hbm, wo_ref, wo_sem)
    wo_copy.start()

    small = jnp.exp(-fg_ref[...])
    series = small * (1.0 - small * (0.5 - small * (1.0 / 3.0 - 0.25 * small)))
    log_forget = -jnp.where(small < 0.01, series, jnp.log(1.0 + small))
    cum = running(log_forget, jnp.add, 0.0)
    level_in = ig_ref[...] - cum
    peak = running(level_in, jnp.maximum, VERY_NEGATIVE)
    total_col = cum[:, length - 1 : length]
    top_col = peak[:, length - 1 : length]
    weight = jnp.exp(level_in - top_col)

    lane_head = lax.broadcasted_iota(jnp.int32, (1, width), 1) // head
    masks = [lane_head == h for h in range(head_count)]

    def spread(column):
        row = jnp.zeros((1, width), F32)
        for h in range(head_count):
            row = jnp.where(masks[h], column[h : h + 1, :], row)
        return row

    total_row = spread(total_col)
    level_row = total_row + spread(top_col)

    k_turned = k_ref[...].astype(F32).T
    parts = [
        k_turned[h * head : (h + 1) * head, :] * weight[h : h + 1, :] for h in range(head_count)
    ]
    high, low = halves(jnp.concatenate(parts, axis=0))
    values = v_ref[...]
    whole = dot(high, values) + dot(low, values)
    memory = jnp.zeros((head, width), F32)
    for h in range(head_count):
        memory = jnp.where(masks[h], whole[h * head : (h + 1) * head, :], memory)
    rows = head // PLANE
    for n in range(PLANE):
        put(s1_ref, n, (total_row, level_row, memory[n * rows : (n + 1) * rows, :]))
    put(r1_ref, place, unpacked(s1_ref, place))

    pl.semaphore_wait(barrier, sp_count - 1 + tp_count - 1)

    def exchange1(step):
        peer = lax.rem(place + step, PLANE)
        return pltpu.make_async_remote_copy(
            src_ref=s1_ref.at[peer],
            dst_ref=r1_ref.at[place],
            send_sem=send1.at[peer],
            recv_sem=recv1.at[place],
            device_id={"sp": zed * PLANE + peer},
            device_id_type=MESH,
        )

    def arrival1(step):
        peer = lax.rem(place + step, PLANE)
        return pltpu.make_async_remote_copy(
            src_ref=s1_ref.at[peer],
            dst_ref=r1_ref.at[peer],
            send_sem=send1.at[peer],
            recv_sem=recv1.at[peer],
            device_id={"sp": zed * PLANE + peer},
            device_id_type=MESH,
        )

    def exchange2(step, at):
        peer = lax.rem(zed + step, planes)
        return pltpu.make_async_remote_copy(
            src_ref=s2_ref.at[0],
            dst_ref=r2_ref.at[peer if at is None else at],
            send_sem=send2.at[peer],
            recv_sem=recv2.at[peer if at is None else at],
            device_id={"sp": peer * PLANE + place},
            device_id_type=MESH,
        )

    def exchange3(step, at):
        peer = lax.rem(place + step, PLANE)
        return pltpu.make_async_remote_copy(
            src_ref=s3_ref.at[peer],
            dst_ref=r3_ref.at[peer if at is None else at],
            send_sem=send3.at[peer],
            recv_sem=recv3.at[peer if at is None else at],
            device_id={"sp": zed * PLANE + peer},
            device_id_type=MESH,
        )

    for step in range(1, PLANE):
        exchange1(step).start()

    peak_cols = jnp.concatenate([peak, jnp.zeros((8 - head_count, length), F32)], axis=0).T
    peak_wide = jnp.zeros((length, width), F32)
    for h in range(head_count):
        peak_wide = jnp.where(masks[h], peak_cols[:, h : h + 1], peak_wide)
    scale = head**-0.5
    block = 128

    def inner(t):
        span = (t + 1) * block
        rows_t = slice(t * block, span)
        query = q_ref[rows_t, :].astype(F32) * scale
        position = lax.broadcasted_iota(jnp.int32, (block, span), 0) + t * block
        source = lax.broadcasted_iota(jnp.int32, (block, span), 1)
        causal = source <= position
        found = jnp.zeros((block, width), F32)
        for h in range(head_count):
            mine = jnp.where(masks[h], query, 0.0).astype(BF16)
            scores = dot_t(mine, k_ref[0:span, :])
            gap = level_in[h : h + 1, 0:span] - peak_cols[rows_t, h : h + 1]
            pairs = scores * jnp.exp(jnp.where(causal, gap, VERY_NEGATIVE))
            pairs_high, pairs_low = halves(pairs)
            part = dot(pairs_high, v_ref[0:span, :]) + dot(pairs_low, v_ref[0:span, :])
            found = jnp.where(masks[h], part, found)
        intra_ref[rows_t, :] = found

    inner(0)
    inner(1)

    for step in range(1, PLANE):
        arrival1(step).wait()
    identity = (
        jnp.zeros((1, width), F32),
        jnp.full((1, width), VERY_NEGATIVE, F32),
        jnp.zeros((rows, width), F32),
    )
    prior = [identity]
    for n in range(PLANE):
        prior.append(join(prior[-1], unpacked(r1_ref, n)))
    put(s2_ref, 0, prior[-1])
    put(r2_ref, zed, prior[-1])
    for step in range(1, planes):
        exchange2(step, zed).start()

    inner(2)

    for step in range(1, planes):
        exchange2(step, None).wait()
    entering = identity
    for n in range(planes):
        later = join(entering, unpacked(r2_ref, n))
        entering = tuple(jnp.where(n < zed, new, old) for new, old in zip(later, entering))
    for n in range(PLANE):
        put(s3_ref, n, join(entering, prior[n]))
    put(r3_ref, place, unpacked(s3_ref, place))
    for step in range(1, PLANE):
        exchange3(step, place).start()

    inner(3)

    for step in range(1, PLANE):
        exchange3(step, None).wait()
    prior_total = r3_ref[0, 8:9, :]
    prior_level = r3_ref[0, 9:10, :]
    start_level = jnp.maximum(prior_level, prior_total)
    opening = jnp.exp(prior_level - start_level)
    began = jnp.concatenate([r3_ref[n, 0:8, :] for n in range(PLANE)], axis=0) * opening
    blocks = jnp.concatenate([jnp.where(masks[h], began, 0.0) for h in range(head_count)], axis=0)
    block_high, block_low = halves(blocks)
    queries = (q_ref[...].astype(F32) * scale).astype(BF16)
    carried = dot(queries, block_high) + dot(queries, block_low)
    level = jnp.maximum(peak_wide, start_level)
    cell = jnp.exp(peak_wide - level) * intra_ref[...] + jnp.exp(start_level - level) * carried
    row_head = lax.broadcasted_iota(jnp.int32, (width, width), 0) // head
    column_head = lax.broadcasted_iota(jnp.int32, (width, width), 1) // head
    averaging = jnp.where(row_head == column_head, 1.0 / head, 0.0).astype(BF16)
    square_high, square_low = halves(cell * cell)
    mean = dot(square_high, averaging) + dot(square_low, averaging)
    gate = 1.0 / (1.0 + jnp.exp(-og_ref[...].astype(F32)))
    mixed = (gate * (cell * lax.rsqrt(mean + EPSILON) * hgain_ref[...])).astype(BF16)
    for n in range(tp_count):
        mix_ref[n] = mixed[n * tokens : (n + 1) * tokens, :]

    def exchange4(step, at):
        peer = lax.rem(mt + step, tp_count)
        return pltpu.make_async_remote_copy(
            src_ref=mix_ref.at[peer],
            dst_ref=mrecv_ref.at[peer if at is None else at],
            send_sem=send4.at[peer],
            recv_sem=recv4.at[peer if at is None else at],
            device_id={"tp": peer},
            device_id_type=MESH,
        )

    for step in range(1, tp_count):
        exchange4(step, mt).start()
    mrecv_ref[mt] = mix_ref[mt]

    routes = routes_ref[:, pl.ds(pl.multiple_of(mt * tokens, tokens), tokens)]
    capacity = send_ref.shape[1]
    slots = sp_count * capacity
    first, second = slots_of(routes, capacity, sp_count)
    slot = lax.broadcasted_iota(jnp.int32, (slots, tokens), 0)
    select = jnp.where((slot == first) | (slot == second), 1.0, 0.0).astype(BF16)

    wo_copy.wait()
    for step in range(1, tp_count):
        exchange4(step, None).wait()
    gathered = jnp.concatenate([mrecv_ref[n] for n in range(tp_count)], axis=1)
    model = wo_ref.shape[1]
    piece = 512
    squares = jnp.zeros((tokens, 1), F32)
    for n in range(model // piece):
        cols = slice(n * piece, (n + 1) * piece)
        projected = dot(gathered, wo_ref[:, cols])
        stream = (res_ref[:, cols].astype(F32) + projected).astype(BF16)
        stream_ref[:, cols] = stream
        stream = stream.astype(F32)
        squares = squares + jnp.sum(stream * stream, axis=1, keepdims=True)
    inverse = lax.rsqrt(squares * (1.0 / model) + EPSILON)
    for n in range(model // piece):
        cols = slice(n * piece, (n + 1) * piece)
        normed = (stream_ref[:, cols].astype(F32) * inverse * ngain_ref[:, cols]).astype(BF16)
        chosen = dot(select, normed).reshape(sp_count, capacity, piece)
        send_ref[:, :, cols] = chosen.astype(BF16)

    own_copy = pltpu.make_async_copy(send_ref.at[me], arrived_ref.at[me], own_sem)
    own_copy.start()

    def dispatch(step, at):
        peer = ring_peer(me, step, sp_count)
        return pltpu.make_async_remote_copy(
            src_ref=send_ref.at[peer],
            dst_ref=arrived_ref.at[peer if at is None else at],
            send_sem=send5.at[peer],
            recv_sem=recv5.at[peer if at is None else at],
            device_id={"sp": peer},
            device_id_type=MESH,
        )

    def go(step, _):
        dispatch(step, me).start()
        return 0

    def done(step, _):
        dispatch(step, None).wait()
        return 0

    lax.fori_loop(1, sp_count, go, 0)
    lax.fori_loop(1, sp_count, done, 0)
    own_copy.wait()


def hidden_kernel(rows_ref, gate_ref, up_ref, hidden_ref):
    rows = rows_ref[...]
    gate = dot(rows, gate_ref[0])
    up = dot(rows, up_ref[0])
    hidden_ref[...] = (gate / (1.0 + jnp.exp(-gate)) * up).astype(BF16)


def back_kernel(
    sp_count,
    tp_count,
    hidden_ref,
    down_ref,
    stream_ref,
    routes_ref,
    group_ref,
    scores_ref,
    out_ref,
    send_ref,
    answer_ref,
    send_sem,
    recv_sem,
):
    me = lax.axis_index("sp")
    mt = lax.axis_index("tp")
    barrier = pltpu.get_barrier_semaphore()

    def greet(step, _):
        pl.semaphore_signal(
            barrier, inc=1, device_id={"sp": ring_peer(me, step, sp_count)}, device_id_type=MESH
        )
        return 0

    lax.fori_loop(1, sp_count, greet, 0)
    capacity = send_ref.shape[1]
    model = send_ref.shape[2]
    slots = sp_count * capacity
    tokens = stream_ref.shape[0]
    piece = 512
    hidden = hidden_ref[...]
    for n in range(model // piece):
        cols = slice(n * piece, (n + 1) * piece)
        result = dot(hidden, down_ref[:, cols]).reshape(sp_count, capacity, piece)
        send_ref[:, :, cols] = result.astype(BF16)
    answer_ref[me] = send_ref[me]
    pl.semaphore_wait(barrier, sp_count - 1)

    def give(step, at):
        peer = ring_peer(me, step, sp_count)
        return pltpu.make_async_remote_copy(
            src_ref=send_ref.at[peer],
            dst_ref=answer_ref.at[peer if at is None else at],
            send_sem=send_sem.at[peer],
            recv_sem=recv_sem.at[peer if at is None else at],
            device_id={"sp": peer},
            device_id_type=MESH,
        )

    def go(step, _):
        give(step, me).start()
        return 0

    def done(step, _):
        give(step, None).wait()
        return 0

    lax.fori_loop(1, sp_count, go, 0)

    own = pl.ds(pl.multiple_of(mt * tokens, tokens), tokens)
    first, second = slots_of(routes_ref[:, own], capacity, sp_count)
    scores = scores_ref[:, own]
    most = jnp.maximum(scores[0:1, :], scores[1:2, :])
    first_exp = jnp.exp(scores[0:1, :] - most)
    second_exp = jnp.exp(scores[1:2, :] - most)
    share = group_ref[:, own] / (first_exp + second_exp)
    slot = lax.broadcasted_iota(jnp.int32, (slots, tokens), 0)
    weights = jnp.where(slot == first, share * first_exp, 0.0)
    weights = jnp.where(slot == second, share * second_exp, weights).T
    weights_high, weights_low = halves(weights)

    lax.fori_loop(1, sp_count, done, 0)
    for n in range(model // piece):
        cols = slice(n * piece, (n + 1) * piece)
        answers = answer_ref[:, :, cols].astype(F32).reshape(slots, piece).astype(BF16)
        mix = dot(weights_high, answers) + dot(weights_low, answers)
        out_ref[:, cols] = (stream_ref[:, cols].astype(F32) + mix).astype(BF16)


def shards(
    residual,
    queries,
    key_vectors,
    value_vectors,
    output_gate,
    input_gate,
    forget_gate,
    head_gain,
    output_weight,
    norm_gain,
    route_experts,
    group_weight,
    expert_scores,
    gate_weight,
    up_weight,
    down_weight,
):
    sp_count = lax.axis_size("sp")
    tp_count = lax.axis_size("tp")
    length, width = queries.shape
    head_count = input_gate.shape[1]
    tokens, model = residual.shape
    capacity = 4 * tokens // sp_count
    hidden_part = gate_weight.shape[2]
    hidden_all = hidden_part * tp_count

    gates = lax.all_gather(gate_weight[0], "tp", axis=0, tiled=False)
    ups = lax.all_gather(up_weight[0], "tp", axis=0, tiled=False)
    downs = lax.all_gather(down_weight[0], "tp", axis=0, tiled=True)

    routes = route_experts.T
    vmem = pl.BlockSpec(memory_space=pltpu.VMEM)
    hbm = pl.BlockSpec(memory_space=pl.ANY)
    dma = pltpu.SemaphoreType.DMA
    planes = sp_count // PLANE
    arrived, stream = pl.pallas_call(
        functools.partial(front_kernel, sp_count, tp_count, head_count),
        out_shape=(
            jax.ShapeDtypeStruct((sp_count, capacity, model), BF16),
            jax.ShapeDtypeStruct((tokens, model), BF16),
        ),
        in_specs=[vmem] * 7 + [hbm] + [vmem] * 3,
        out_specs=(hbm, vmem),
        scratch_shapes=[
            pltpu.VMEM(output_weight.shape, BF16),
            pltpu.VMEM((length, width), F32),
            pltpu.VMEM((PLANE, 16, width), F32),
            pltpu.VMEM((PLANE, 16, width), F32),
            pltpu.VMEM((1, 16, width), F32),
            pltpu.VMEM((planes, 16, width), F32),
            pltpu.VMEM((PLANE, 16, width), F32),
            pltpu.VMEM((PLANE, 16, width), F32),
            pltpu.VMEM((tp_count, tokens, width), BF16),
            pltpu.VMEM((tp_count, tokens, width), BF16),
            pltpu.VMEM((sp_count, capacity, model), BF16),
            dma,
            dma,
            dma((PLANE,)),
            dma((PLANE,)),
            dma((planes,)),
            dma((planes,)),
            dma((PLANE,)),
            dma((PLANE,)),
            dma((tp_count,)),
            dma((tp_count,)),
            dma((sp_count,)),
            dma((sp_count,)),
        ],
        compiler_params=pltpu.CompilerParams(
            collective_id=0, has_side_effects=True, vmem_limit_bytes=40 * 2**20
        ),
        cost_estimate=pl.CostEstimate(
            flops=60_000_000_000, bytes_accessed=10_000_000, transcendentals=0
        ),
    )(
        queries,
        key_vectors,
        value_vectors,
        output_gate,
        input_gate.T,
        forget_gate.T,
        head_gain.reshape(1, width),
        output_weight,
        residual,
        norm_gain.reshape(1, model),
        routes,
    )

    slots = sp_count * capacity
    hidden = pl.pallas_call(
        hidden_kernel,
        grid=(tp_count,),
        out_shape=jax.ShapeDtypeStruct((slots, hidden_all), BF16),
        in_specs=[
            pl.BlockSpec((slots, model), lambda n: (0, 0)),
            pl.BlockSpec((1, model, hidden_part), lambda n: (n, 0, 0)),
            pl.BlockSpec((1, model, hidden_part), lambda n: (n, 0, 0)),
        ],
        out_specs=pl.BlockSpec((slots, hidden_part), lambda n: (0, n)),
        compiler_params=pltpu.CompilerParams(vmem_limit_bytes=40 * 2**20),
        cost_estimate=pl.CostEstimate(
            flops=4 * slots * model * hidden_all,
            bytes_accessed=4 * model * hidden_all,
            transcendentals=slots * hidden_all,
        ),
    )(arrived.reshape(slots, model), gates, ups)

    return pl.pallas_call(
        functools.partial(back_kernel, sp_count, tp_count),
        out_shape=jax.ShapeDtypeStruct((tokens, model), BF16),
        in_specs=[vmem] * 6,
        out_specs=vmem,
        scratch_shapes=[
            pltpu.VMEM((sp_count, capacity, model), BF16),
            pltpu.VMEM((sp_count, capacity, model), BF16),
            dma((sp_count,)),
            dma((sp_count,)),
        ],
        compiler_params=pltpu.CompilerParams(
            collective_id=1, has_side_effects=True, vmem_limit_bytes=40 * 2**20
        ),
        cost_estimate=pl.CostEstimate(
            flops=60_000_000_000, bytes_accessed=10_000_000, transcendentals=0
        ),
    )(hidden, downs, stream, routes, group_weight.reshape(1, length), expert_scores.T)


def solution(mesh):
    both = ("sp", "tp")
    return jax.shard_map(
        shards,
        mesh=mesh,
        in_specs=(
            P(both, None),
            P("sp", "tp"),
            P("sp", "tp"),
            P("sp", "tp"),
            P("sp", "tp"),
            P("sp", "tp"),
            P("sp", "tp"),
            P("tp", None),
            P(),
            P(),
            P("sp", None),
            P("sp"),
            P("sp", None),
            P("sp", None, "tp"),
            P("sp", None, "tp"),
            P("sp", "tp", None),
        ),
        out_specs=P(both, None),
        check_vma=False,
    )
```

```python
import functools

import jax
import jax.numpy as jnp
from jax import lax
from jax.experimental import pallas as pl
from jax.experimental.pallas import tpu as pltpu
from jax.sharding import PartitionSpec as P

EPSILON = 1e-06
VERY_NEGATIVE = -1e30
MESH = pl.DeviceIdType.MESH
PLANE = 8
F32 = jnp.float32
BF16 = jnp.bfloat16


def dot(a, b):
    return jnp.dot(a, b, preferred_element_type=F32)


def dot_t(a, b):
    return lax.dot_general(a, b, (((1,), (1,)), ((), ())), preferred_element_type=F32)


def halves(x):
    high = x.astype(BF16)
    return high, (x - high.astype(F32)).astype(BF16)


def shifted(x, by, fill):
    lane = lax.broadcasted_iota(jnp.int32, x.shape, 1)
    return jnp.where(lane >= by, pltpu.roll(x, by, 1), fill)


def running(x, combine, fill):
    by = 1
    while by < x.shape[1]:
        x = combine(x, shifted(x, by, fill))
        by *= 2
    return x


def join(early, late):
    early_total, early_level, early_memory = early
    late_total, late_level, late_memory = late
    level = jnp.maximum(late_total + early_level, late_level)
    memory = (
        jnp.exp(late_total + early_level - level) * early_memory
        + jnp.exp(late_level - level) * late_memory
    )
    return early_total + late_total, level, memory


def packed(total, level, memory):
    row = lax.broadcasted_iota(jnp.int32, memory.shape, 0)
    return memory, jnp.where(row == 0, total, jnp.where(row == 1, level, 0.0))


def unpacked(ref, index):
    return ref[index, 8:9, :], ref[index, 9:10, :], ref[index, 0:8, :]


def put(ref, index, state):
    memory, scalars = packed(*state)
    ref[index, 0:8, :] = memory
    ref[index, 8:16, :] = scalars


def ring_peer(me, step, count):
    away = (step + 1) // 2
    sign = 2 * lax.rem(step, 2) - 1
    return lax.rem(me + sign * away + count, count)


def slots_of(routes, capacity, experts):
    tokens = routes.shape[1]
    expert = lax.broadcasted_iota(jnp.int32, (experts, tokens), 0)
    first = expert == routes[0:1, :]
    second = expert == routes[1:2, :]
    row = lax.broadcasted_iota(jnp.int32, (tokens, tokens), 0)
    column = lax.broadcasted_iota(jnp.int32, (tokens, tokens), 1)
    earlier = jnp.where(row < column, 1.0, 0.0).astype(BF16)
    ones = jnp.ones((tokens, tokens), BF16)
    first_hot = jnp.where(first, 1.0, 0.0).astype(BF16)
    second_hot = jnp.where(second, 1.0, 0.0).astype(BF16)
    first_rank = dot(first_hot, earlier)
    second_rank = dot(first_hot, ones) + dot(second_hot, earlier)
    places = []
    for hot, rank, route in ((first, first_rank, routes[0:1, :]), (second, second_rank, routes[1:2, :])):
        own = jnp.sum(jnp.where(hot, rank, 0.0), axis=0, keepdims=True)
        places.append(route * capacity + own.astype(jnp.int32))
    return places


class Ring:
    def __init__(self, ref, item, me, count, sends, arrivals):
        self.ref, self.item, self.me, self.count = ref, item, me, count
        self.sends, self.arrivals = sends, arrivals
        self.half = ref.shape[1] // 2

    def copy(self, kind):
        right = lax.rem(self.me + 1, self.count)
        left = lax.rem(self.me + self.count - 1, self.count)
        first, last = pl.ds(0, self.half), pl.ds(self.half, self.half)
        source, target = (
            (self.ref.at[self.me], right),
            (self.ref.at[self.me], left),
            (self.ref.at[left, first], right),
            (self.ref.at[right, last], left),
        )[kind]
        return pltpu.make_async_remote_copy(
            src_ref=source,
            dst_ref=source,
            send_sem=self.sends.at[self.item, kind],
            recv_sem=self.arrivals.at[self.item, kind],
            device_id={"tp": target},
            device_id_type=MESH,
        )

    def arrival(self, kind):
        right = lax.rem(self.me + 1, self.count)
        left = lax.rem(self.me + self.count - 1, self.count)
        across = lax.rem(self.me + 2, self.count)
        first, last = pl.ds(0, self.half), pl.ds(self.half, self.half)
        source, landed = (
            (self.ref.at[self.me], self.ref.at[left]),
            (self.ref.at[self.me], self.ref.at[right]),
            (self.ref.at[left, first], self.ref.at[across, first]),
            (self.ref.at[right, last], self.ref.at[across, last]),
        )[kind]
        return pltpu.make_async_remote_copy(
            src_ref=source,
            dst_ref=landed,
            send_sem=self.sends.at[self.item, kind],
            recv_sem=self.arrivals.at[self.item, kind],
            device_id={"tp": right},
            device_id_type=MESH,
        )

    def start(self):
        self.copy(0).start()
        self.copy(1).start()

    def forward(self):
        self.arrival(0).wait_recv()
        self.copy(2).start()
        self.arrival(1).wait_recv()
        self.copy(3).start()

    def complete(self):
        self.arrival(2).wait_recv()
        self.arrival(3).wait_recv()

    def sent(self):
        for kind in range(4):
            self.copy(kind).wait_send()


def layer_kernel(sp_count, tp_count, head_count, *refs):
    (
        q_hbm,
        k_hbm,
        v_hbm,
        og_hbm,
        ig_hbm,
        fg_hbm,
        hgain_hbm,
        wo_hbm,
        res_hbm,
        ngain_hbm,
        routes_hbm,
        group_hbm,
        scores_hbm,
        gate_hbm,
        up_hbm,
        down_hbm,
        out_ref,
        q_ref,
        k_ref,
        v_ref,
        og_ref,
        ig_ref,
        fg_ref,
        hgain_ref,
        wo_ref,
        res_ref,
        ngain_ref,
        routes_ref,
        group_ref,
        scores_ref,
        gate_ref,
        up_ref,
        down_a_ref,
        down_b_ref,
        intra_ref,
        s1_ref,
        r1_ref,
        s2_ref,
        r2_ref,
        s3_ref,
        r3_ref,
        mix_ref,
        mrecv_ref,
        stream_ref,
        send_ref,
        arrived_ref,
        hidden_ref,
        back_ref,
        answer_ref,
        load_sem,
        send1,
        recv1,
        send2,
        recv2,
        send3,
        recv3,
        send4,
        recv4,
        send5,
        recv5,
        send6,
        recv6,
        ring_send,
        ring_recv,
    ) = refs
    me = lax.axis_index("sp")
    mt = lax.axis_index("tp")
    zed = me // PLANE
    place = lax.rem(me, PLANE)
    planes = sp_count // PLANE
    length, width = q_ref.shape
    head = width // head_count
    tokens = length // tp_count
    capacity = send_ref.shape[1]
    model = send_ref.shape[2]
    slots = sp_count * capacity
    column_half = model // 2

    loads = [
        (fg_hbm, fg_ref),
        (ig_hbm, ig_ref),
        (k_hbm, k_ref),
        (v_hbm, v_ref),
        (q_hbm, q_ref),
        (gate_hbm.at[0], gate_ref.at[mt]),
        (og_hbm, og_ref),
        (hgain_hbm, hgain_ref),
        (ngain_hbm, ngain_ref),
        (routes_hbm, routes_ref),
        (group_hbm, group_ref),
        (scores_hbm, scores_ref),
        (res_hbm, res_ref),
        (up_hbm.at[0], up_ref.at[mt]),
        (wo_hbm, wo_ref),
        (down_hbm.at[0, :, pl.ds(0, column_half)], down_a_ref.at[mt]),
        (down_hbm.at[0, :, pl.ds(column_half, column_half)], down_b_ref.at[mt]),
    ]
    loads = [
        pltpu.make_async_copy(source, target, load_sem.at[n])
        for n, (source, target) in enumerate(loads)
    ]
    for load in loads:
        load.start()

    barrier = pltpu.get_barrier_semaphore()

    def greet(step, _):
        pl.semaphore_signal(
            barrier, inc=1, device_id={"sp": ring_peer(me, step, sp_count)}, device_id_type=MESH
        )
        return 0

    lax.fori_loop(1, sp_count, greet, 0)

    def greet_tp(step, _):
        pl.semaphore_signal(
            barrier, inc=1, device_id={"tp": lax.rem(mt + step, tp_count)}, device_id_type=MESH
        )
        return 0

    lax.fori_loop(1, tp_count, greet_tp, 0)

    gate_ring, up_ring, down_a_ring, down_b_ring = [
        Ring(ref, item, mt, tp_count, ring_send, ring_recv)
        for item, ref in enumerate((gate_ref, up_ref, down_a_ref, down_b_ref))
    ]
    for load in loads[:6]:
        load.wait()

    small = jnp.exp(-fg_ref[...])
    series = small * (1.0 - small * (0.5 - small * (1.0 / 3.0 - 0.25 * small)))
    log_forget = -jnp.where(small < 0.01, series, jnp.log(1.0 + small))
    cum = running(log_forget, jnp.add, 0.0)
    level_in = ig_ref[...] - cum
    peak = running(level_in, jnp.maximum, VERY_NEGATIVE)
    total_col = cum[:, length - 1 : length]
    top_col = peak[:, length - 1 : length]
    weight = jnp.exp(level_in - top_col)

    lane_head = lax.broadcasted_iota(jnp.int32, (1, width), 1) // head
    masks = [lane_head == h for h in range(head_count)]

    def spread(column):
        row = jnp.zeros((1, width), F32)
        for h in range(head_count):
            row = jnp.where(masks[h], column[h : h + 1, :], row)
        return row

    total_row = spread(total_col)
    level_row = total_row + spread(top_col)

    k_turned = k_ref[...].astype(F32).T
    parts = [
        k_turned[h * head : (h + 1) * head, :] * weight[h : h + 1, :] for h in range(head_count)
    ]
    high, low = halves(jnp.concatenate(parts, axis=0))
    values = v_ref[...]
    whole = dot(high, values) + dot(low, values)
    memory = jnp.zeros((head, width), F32)
    for h in range(head_count):
        memory = jnp.where(masks[h], whole[h * head : (h + 1) * head, :], memory)
    rows = head // PLANE
    for n in range(PLANE):
        put(s1_ref, n, (total_row, level_row, memory[n * rows : (n + 1) * rows, :]))
    put(r1_ref, place, unpacked(s1_ref, place))

    pl.semaphore_wait(barrier, sp_count - 1 + tp_count - 1)

    def exchange1(step):
        peer = lax.rem(place + step, PLANE)
        return pltpu.make_async_remote_copy(
            src_ref=s1_ref.at[peer],
            dst_ref=r1_ref.at[place],
            send_sem=send1.at[peer],
            recv_sem=recv1.at[place],
            device_id={"sp": zed * PLANE + peer},
            device_id_type=MESH,
        )

    def arrival1(step):
        peer = lax.rem(place + step, PLANE)
        return pltpu.make_async_remote_copy(
            src_ref=s1_ref.at[peer],
            dst_ref=r1_ref.at[peer],
            send_sem=send1.at[peer],
            recv_sem=recv1.at[peer],
            device_id={"sp": zed * PLANE + peer},
            device_id_type=MESH,
        )

    def exchange2(step, at):
        peer = lax.rem(zed + step, planes)
        return pltpu.make_async_remote_copy(
            src_ref=s2_ref.at[0],
            dst_ref=r2_ref.at[peer if at is None else at],
            send_sem=send2.at[peer],
            recv_sem=recv2.at[peer if at is None else at],
            device_id={"sp": peer * PLANE + place},
            device_id_type=MESH,
        )

    def exchange3(step, at):
        peer = lax.rem(place + step, PLANE)
        return pltpu.make_async_remote_copy(
            src_ref=s3_ref.at[peer],
            dst_ref=r3_ref.at[peer if at is None else at],
            send_sem=send3.at[peer],
            recv_sem=recv3.at[peer if at is None else at],
            device_id={"sp": zed * PLANE + peer},
            device_id_type=MESH,
        )

    for step in range(1, PLANE):
        exchange1(step).start()
    gate_ring.start()

    peak_cols = jnp.concatenate([peak, jnp.zeros((8 - head_count, length), F32)], axis=0).T
    peak_wide = jnp.zeros((length, width), F32)
    for h in range(head_count):
        peak_wide = jnp.where(masks[h], peak_cols[:, h : h + 1], peak_wide)
    scale = head**-0.5
    block = 128

    def inner(t):
        span = (t + 1) * block
        rows_t = slice(t * block, span)
        query = q_ref[rows_t, :].astype(F32) * scale
        position = lax.broadcasted_iota(jnp.int32, (block, span), 0) + t * block
        source = lax.broadcasted_iota(jnp.int32, (block, span), 1)
        causal = source <= position
        found = jnp.zeros((block, width), F32)
        for h in range(head_count):
            mine = jnp.where(masks[h], query, 0.0).astype(BF16)
            scores = dot_t(mine, k_ref[0:span, :])
            gap = level_in[h : h + 1, 0:span] - peak_cols[rows_t, h : h + 1]
            pairs = scores * jnp.exp(jnp.where(causal, gap, VERY_NEGATIVE))
            pairs_high, pairs_low = halves(pairs)
            part = dot(pairs_high, v_ref[0:span, :]) + dot(pairs_low, v_ref[0:span, :])
            found = jnp.where(masks[h], part, found)
        intra_ref[rows_t, :] = found

    inner(0)
    inner(1)

    for step in range(1, PLANE):
        arrival1(step).wait()
    identity = (
        jnp.zeros((1, width), F32),
        jnp.full((1, width), VERY_NEGATIVE, F32),
        jnp.zeros((rows, width), F32),
    )
    prior = [identity]
    for n in range(PLANE):
        prior.append(join(prior[-1], unpacked(r1_ref, n)))
    put(s2_ref, 0, prior[-1])
    put(r2_ref, zed, prior[-1])
    for step in range(1, planes):
        exchange2(step, zed).start()

    inner(2)

    for step in range(1, planes):
        exchange2(step, None).wait()
    entering = identity
    for n in range(planes):
        later = join(entering, unpacked(r2_ref, n))
        entering = tuple(jnp.where(n < zed, new, old) for new, old in zip(later, entering))
    for n in range(PLANE):
        put(s3_ref, n, join(entering, prior[n]))
    put(r3_ref, place, unpacked(s3_ref, place))
    for step in range(1, PLANE):
        exchange3(step, place).start()

    inner(3)

    for step in range(1, PLANE):
        exchange3(step, None).wait()
    prior_total = r3_ref[0, 8:9, :]
    prior_level = r3_ref[0, 9:10, :]
    start_level = jnp.maximum(prior_level, prior_total)
    opening = jnp.exp(prior_level - start_level)
    began = jnp.concatenate([r3_ref[n, 0:8, :] for n in range(PLANE)], axis=0) * opening
    blocks = jnp.concatenate([jnp.where(masks[h], began, 0.0) for h in range(head_count)], axis=0)
    block_high, block_low = halves(blocks)
    queries = (q_ref[...].astype(F32) * scale).astype(BF16)
    carried = dot(queries, block_high) + dot(queries, block_low)
    level = jnp.maximum(peak_wide, start_level)
    cell = jnp.exp(peak_wide - level) * intra_ref[...] + jnp.exp(start_level - level) * carried
    row_head = lax.broadcasted_iota(jnp.int32, (width, width), 0) // head
    column_head = lax.broadcasted_iota(jnp.int32, (width, width), 1) // head
    averaging = jnp.where(row_head == column_head, 1.0 / head, 0.0).astype(BF16)
    square_high, square_low = halves(cell * cell)
    mean = dot(square_high, averaging) + dot(square_low, averaging)
    for load in loads[6:]:
        load.wait()
    gain = jnp.concatenate([hgain_ref[h : h + 1, :] for h in range(head_count)], axis=1)
    gate = 1.0 / (1.0 + jnp.exp(-og_ref[...].astype(F32)))
    mixed = (gate * (cell * lax.rsqrt(mean + EPSILON) * gain)).astype(BF16)
    for n in range(tp_count):
        mix_ref[n] = mixed[n * tokens : (n + 1) * tokens, :]

    def exchange4(step, at):
        peer = lax.rem(mt + step, tp_count)
        return pltpu.make_async_remote_copy(
            src_ref=mix_ref.at[peer],
            dst_ref=mrecv_ref.at[peer if at is None else at],
            send_sem=send4.at[peer],
            recv_sem=recv4.at[peer if at is None else at],
            device_id={"tp": peer},
            device_id_type=MESH,
        )

    for step in range(1, tp_count):
        exchange4(step, mt).start()
    up_ring.start()
    mrecv_ref[mt] = mix_ref[mt]

    routes = routes_ref[:, pl.ds(pl.multiple_of(mt * tokens, tokens), tokens)]
    first, second = slots_of(routes, capacity, sp_count)
    slot = lax.broadcasted_iota(jnp.int32, (slots, tokens), 0)
    select = jnp.where((slot == first) | (slot == second), 1.0, 0.0).astype(BF16)

    for step in range(1, tp_count):
        exchange4(step, None).wait()
    gathered = jnp.concatenate([mrecv_ref[n] for n in range(tp_count)], axis=1)
    piece = 512
    squares = jnp.zeros((tokens, 1), F32)
    for n in range(model // piece):
        cols = slice(n * piece, (n + 1) * piece)
        projected = dot(gathered, wo_ref[:, cols])
        stream = (res_ref[:, cols].astype(F32) + projected).astype(BF16)
        stream_ref[:, cols] = stream
        stream = stream.astype(F32)
        squares = squares + jnp.sum(stream * stream, axis=1, keepdims=True)
    inverse = lax.rsqrt(squares * (1.0 / model) + EPSILON)
    for n in range(model // piece):
        cols = slice(n * piece, (n + 1) * piece)
        normed = (stream_ref[:, cols].astype(F32) * inverse * ngain_ref[:, cols]).astype(BF16)
        chosen = dot(select, normed).reshape(sp_count, capacity, piece)
        send_ref[:, :, cols] = chosen.astype(BF16)

    arrived_ref[me] = send_ref[me]

    def dispatch(step, at):
        peer = ring_peer(me, step, sp_count)
        return pltpu.make_async_remote_copy(
            src_ref=send_ref.at[peer],
            dst_ref=arrived_ref.at[peer if at is None else at],
            send_sem=send5.at[peer],
            recv_sem=recv5.at[peer if at is None else at],
            device_id={"sp": peer},
            device_id_type=MESH,
        )

    def go(step, _):
        dispatch(step, me).start()
        return 0

    def done(step, _):
        dispatch(step, None).wait()
        return 0

    lax.fori_loop(1, sp_count, go, 0)
    gate_ring.forward()

    own = pl.ds(pl.multiple_of(mt * tokens, tokens), tokens)
    scores = scores_ref[:, own]
    most = jnp.maximum(scores[0:1, :], scores[1:2, :])
    first_exp = jnp.exp(scores[0:1, :] - most)
    second_exp = jnp.exp(scores[1:2, :] - most)
    share = group_ref[:, own] / (first_exp + second_exp)
    weights = jnp.where(slot == first, share * first_exp, 0.0)
    weights = jnp.where(slot == second, share * second_exp, weights).T
    weights_high, weights_low = halves(weights)

    up_ring.forward()
    down_a_ring.start()
    lax.fori_loop(1, sp_count, done, 0)
    gate_ring.complete()
    up_ring.complete()

    def expert(n, _):
        rows_in = arrived_ref.reshape(slots, model)[...]
        gated = dot(rows_in, gate_ref[n])
        raised = dot(rows_in, up_ref[n])
        hidden_ref[n] = (gated / (1.0 + jnp.exp(-gated)) * raised).astype(BF16)
        return 0

    lax.fori_loop(0, tp_count, expert, 0)

    wide = 256

    def answer(half, down_ref):
        def some(n, _):
            cols = pl.ds(pl.multiple_of(n * wide, wide), wide)
            result = jnp.zeros((slots, wide), F32)
            for quarter in range(tp_count):
                result = result + dot(hidden_ref[quarter], down_ref[quarter, :, cols])
            back_ref[half, :, :, cols] = result.reshape(sp_count, capacity, wide).astype(BF16)
            return 0

        lax.fori_loop(0, column_half // wide, some, 0)
        answer_ref[half, me] = back_ref[half, me]

        def go(step, _):
            give(half, step, me).start()
            return 0

        lax.fori_loop(1, sp_count, go, 0)

    def give(half, step, at):
        peer = ring_peer(me, step, sp_count)
        return pltpu.make_async_remote_copy(
            src_ref=back_ref.at[half, peer],
            dst_ref=answer_ref.at[half, peer if at is None else at],
            send_sem=send6.at[half, peer],
            recv_sem=recv6.at[half, peer if at is None else at],
            device_id={"sp": peer},
            device_id_type=MESH,
        )

    def finish(half):
        def done(step, _):
            give(half, step, None).wait()
            return 0

        lax.fori_loop(1, sp_count, done, 0)
        part = answer_ref.at[half].reshape(slots, column_half)
        for n in range(column_half // piece):
            answers = part[:, n * piece : (n + 1) * piece]
            mix = dot(weights_high, answers) + dot(weights_low, answers)
            cols = slice(half * column_half + n * piece, half * column_half + (n + 1) * piece)
            out_ref[:, cols] = (stream_ref[:, cols].astype(F32) + mix).astype(BF16)

    down_a_ring.forward()
    down_b_ring.start()
    down_a_ring.complete()
    answer(0, down_a_ref)
    down_b_ring.forward()
    down_b_ring.complete()
    answer(1, down_b_ref)
    finish(0)
    finish(1)
    for ring in (gate_ring, up_ring, down_a_ring, down_b_ring):
        ring.sent()


def shards(
    residual,
    queries,
    key_vectors,
    value_vectors,
    output_gate,
    input_gate,
    forget_gate,
    head_gain,
    output_weight,
    norm_gain,
    route_experts,
    group_weight,
    expert_scores,
    gate_weight,
    up_weight,
    down_weight,
):
    sp_count = lax.axis_size("sp")
    tp_count = lax.axis_size("tp")
    length, width = queries.shape
    head_count, head = input_gate.shape[1], head_gain.shape[1]
    tokens, model = residual.shape
    capacity = 4 * tokens // sp_count
    hidden_part = gate_weight.shape[2]
    planes = sp_count // PLANE
    slots = sp_count * capacity
    dma = pltpu.SemaphoreType.DMA
    vmem = pltpu.VMEM
    return pl.pallas_call(
        functools.partial(layer_kernel, sp_count, tp_count, head_count),
        out_shape=jax.ShapeDtypeStruct((tokens, model), BF16),
        in_specs=[pl.BlockSpec(memory_space=pl.ANY)] * 16,
        out_specs=pl.BlockSpec(memory_space=pltpu.VMEM),
        scratch_shapes=[
            vmem((length, width), BF16),
            vmem((length, width), BF16),
            vmem((length, width), BF16),
            vmem((length, width), BF16),
            vmem((head_count, length), F32),
            vmem((head_count, length), F32),
            vmem((head_count, head), F32),
            vmem(output_weight.shape, BF16),
            vmem((tokens, model), BF16),
            vmem((1, model), F32),
            vmem((2, length), jnp.int32),
            vmem((1, length), F32),
            vmem((2, length), F32),
            vmem((tp_count, model, hidden_part), BF16),
            vmem((tp_count, model, hidden_part), BF16),
            vmem((tp_count, hidden_part, model // 2), BF16),
            vmem((tp_count, hidden_part, model // 2), BF16),
            vmem((length, width), F32),
            vmem((PLANE, 16, width), F32),
            vmem((PLANE, 16, width), F32),
            vmem((1, 16, width), F32),
            vmem((planes, 16, width), F32),
            vmem((PLANE, 16, width), F32),
            vmem((PLANE, 16, width), F32),
            vmem((tp_count, tokens, width), BF16),
            vmem((tp_count, tokens, width), BF16),
            vmem((tokens, model), BF16),
            vmem((sp_count, capacity, model), BF16),
            vmem((sp_count, capacity, model), BF16),
            vmem((tp_count, slots, hidden_part), BF16),
            vmem((2, sp_count, capacity, model // 2), BF16),
            vmem((2, sp_count, capacity, model // 2), BF16),
            dma((17,)),
            dma((PLANE,)),
            dma((PLANE,)),
            dma((planes,)),
            dma((planes,)),
            dma((PLANE,)),
            dma((PLANE,)),
            dma((tp_count,)),
            dma((tp_count,)),
            dma((sp_count,)),
            dma((sp_count,)),
            dma((2, sp_count)),
            dma((2, sp_count)),
            dma((4, 4)),
            dma((4, 4)),
        ],
        compiler_params=pltpu.CompilerParams(
            collective_id=0, has_side_effects=True, vmem_limit_bytes=66_000_000
        ),
    )(
        queries,
        key_vectors,
        value_vectors,
        output_gate,
        input_gate.T,
        forget_gate.T,
        head_gain,
        output_weight,
        residual,
        norm_gain.reshape(1, model),
        route_experts.T,
        group_weight.reshape(1, length),
        expert_scores.T,
        gate_weight,
        up_weight,
        down_weight,
    )


def solution(mesh):
    both = ("sp", "tp")
    return jax.shard_map(
        shards,
        mesh=mesh,
        in_specs=(
            P(both, None),
            P("sp", "tp"),
            P("sp", "tp"),
            P("sp", "tp"),
            P("sp", "tp"),
            P("sp", "tp"),
            P("sp", "tp"),
            P("tp", None),
            P(),
            P(),
            P("sp", None),
            P("sp"),
            P("sp", None),
            P("sp", None, "tp"),
            P("sp", None, "tp"),
            P("sp", "tp", None),
        ),
        out_specs=P(both, None),
        check_vma=False,
    )
```

```python
import functools

import jax
import jax.numpy as jnp
from jax import lax
from jax.experimental import pallas as pl
from jax.experimental.pallas import tpu as pltpu
from jax.sharding import PartitionSpec as P

EPSILON = 1e-06
VERY_NEGATIVE = -1e30
MESH = pl.DeviceIdType.MESH
PLANE = 8
WIDTHS = (256, 256, 512, 512, 512)
F32 = jnp.float32
BF16 = jnp.bfloat16


def dot(a, b):
    return jnp.dot(a, b, preferred_element_type=F32)


def dot_t(a, b):
    return lax.dot_general(a, b, (((1,), (1,)), ((), ())), preferred_element_type=F32)


def halves(x):
    high = x.astype(BF16)
    return high, (x - high.astype(F32)).astype(BF16)


def shifted(x, by, fill):
    lane = lax.broadcasted_iota(jnp.int32, x.shape, 1)
    return jnp.where(lane >= by, pltpu.roll(x, by, 1), fill)


def running(x, combine, fill):
    by = 1
    while by < x.shape[1]:
        x = combine(x, shifted(x, by, fill))
        by *= 2
    return x


def join(early, late):
    early_total, early_level, early_memory = early
    late_total, late_level, late_memory = late
    level = jnp.maximum(late_total + early_level, late_level)
    memory = (
        jnp.exp(late_total + early_level - level) * early_memory
        + jnp.exp(late_level - level) * late_memory
    )
    return early_total + late_total, level, memory


def packed(total, level, memory):
    row = lax.broadcasted_iota(jnp.int32, memory.shape, 0)
    return memory, jnp.where(row == 0, total, jnp.where(row == 1, level, 0.0))


def unpacked(ref, index):
    return ref[index, 8:9, :], ref[index, 9:10, :], ref[index, 0:8, :]


def put(ref, index, state):
    memory, scalars = packed(*state)
    ref[index, 0:8, :] = memory
    ref[index, 8:16, :] = scalars


def ring_peer(me, step, count):
    away = (step + 1) // 2
    sign = 2 * lax.rem(step, 2) - 1
    return lax.rem(me + sign * away + count, count)


def ring_source(me, step, count):
    away = (step + 1) // 2
    sign = 2 * lax.rem(step, 2) - 1
    return lax.rem(me - sign * away + count, count)


def slots_of(routes, capacity, experts):
    tokens = routes.shape[1]
    expert = lax.broadcasted_iota(jnp.int32, (experts, tokens), 0)
    first = expert == routes[0:1, :]
    second = expert == routes[1:2, :]
    row = lax.broadcasted_iota(jnp.int32, (tokens, tokens), 0)
    column = lax.broadcasted_iota(jnp.int32, (tokens, tokens), 1)
    earlier = jnp.where(row < column, 1.0, 0.0).astype(BF16)
    ones = jnp.ones((tokens, tokens), BF16)
    first_hot = jnp.where(first, 1.0, 0.0).astype(BF16)
    second_hot = jnp.where(second, 1.0, 0.0).astype(BF16)
    first_rank = dot(first_hot, earlier)
    second_rank = dot(first_hot, ones) + dot(second_hot, earlier)
    places = []
    for hot, rank, route in ((first, first_rank, routes[0:1, :]), (second, second_rank, routes[1:2, :])):
        own = jnp.sum(jnp.where(hot, rank, 0.0), axis=0, keepdims=True)
        places.append(route * capacity + own.astype(jnp.int32))
    return places


class Ring:
    def __init__(self, ref, item, me, count, sends, arrivals):
        self.ref, self.item, self.me, self.count = ref, item, me, count
        self.sends, self.arrivals = sends, arrivals
        self.half = ref.shape[1] // 2

    def copy(self, kind):
        right = lax.rem(self.me + 1, self.count)
        left = lax.rem(self.me + self.count - 1, self.count)
        first, last = pl.ds(0, self.half), pl.ds(self.half, self.half)
        source, target = (
            (self.ref.at[self.me], right),
            (self.ref.at[self.me], left),
            (self.ref.at[left, first], right),
            (self.ref.at[right, last], left),
        )[kind]
        return pltpu.make_async_remote_copy(
            src_ref=source,
            dst_ref=source,
            send_sem=self.sends.at[self.item, kind],
            recv_sem=self.arrivals.at[self.item, kind],
            device_id={"tp": target},
            device_id_type=MESH,
        )

    def arrival(self, kind):
        right = lax.rem(self.me + 1, self.count)
        left = lax.rem(self.me + self.count - 1, self.count)
        across = lax.rem(self.me + 2, self.count)
        first, last = pl.ds(0, self.half), pl.ds(self.half, self.half)
        source, landed = (
            (self.ref.at[self.me], self.ref.at[left]),
            (self.ref.at[self.me], self.ref.at[right]),
            (self.ref.at[left, first], self.ref.at[across, first]),
            (self.ref.at[right, last], self.ref.at[across, last]),
        )[kind]
        return pltpu.make_async_remote_copy(
            src_ref=source,
            dst_ref=landed,
            send_sem=self.sends.at[self.item, kind],
            recv_sem=self.arrivals.at[self.item, kind],
            device_id={"tp": right},
            device_id_type=MESH,
        )

    def start(self):
        self.copy(0).start()
        self.copy(1).start()

    def forward(self):
        self.arrival(0).wait_recv()
        self.copy(2).start()
        self.arrival(1).wait_recv()
        self.copy(3).start()

    def complete(self):
        self.arrival(2).wait_recv()
        self.arrival(3).wait_recv()

    def sent(self):
        for kind in range(4):
            self.copy(kind).wait_send()


def layer_kernel(sp_count, tp_count, head_count, *refs):
    chunks = len(WIDTHS)
    starts = [sum(WIDTHS[:n]) for n in range(chunks)]
    listed = refs[len(refs) - 3 * chunks :]
    refs = refs[: len(refs) - 3 * chunks]
    back_refs, answer_refs = listed[:chunks], listed[chunks : 2 * chunks]
    down_refs = listed[2 * chunks :]
    (
        q_hbm,
        k_hbm,
        v_hbm,
        og_hbm,
        ig_hbm,
        fg_hbm,
        hgain_hbm,
        wo_hbm,
        res_hbm,
        ngain_hbm,
        routes_hbm,
        group_hbm,
        scores_hbm,
        gate_hbm,
        up_hbm,
        down_hbm,
        out_ref,
        q_ref,
        k_ref,
        v_ref,
        og_ref,
        ig_ref,
        fg_ref,
        hgain_ref,
        wo_ref,
        res_ref,
        ngain_ref,
        routes_ref,
        group_ref,
        scores_ref,
        gate_ref,
        up_ref,
        intra_ref,
        peak_ref,
        s1_ref,
        r1_ref,
        s2_ref,
        r2_ref,
        s3_ref,
        r3_ref,
        mix_ref,
        mrecv_ref,
        stream_ref,
        send_ref,
        arrived_ref,
        hidden_ref,
        load_sem,
        send1,
        recv1,
        send2,
        recv2,
        send3,
        recv3,
        send4,
        recv4,
        send5,
        recv5,
        send6,
        recv6,
        ring_send,
        ring_recv,
    ) = refs
    me = lax.axis_index("sp")
    mt = lax.axis_index("tp")
    zed = me // PLANE
    place = lax.rem(me, PLANE)
    planes = sp_count // PLANE
    length, width = q_ref.shape
    head = width // head_count
    tokens = length // tp_count
    capacity = send_ref.shape[1]
    model = send_ref.shape[2]
    slots = sp_count * capacity

    barrier = pltpu.get_barrier_semaphore()

    loads = [
        (fg_hbm, fg_ref),
        (ig_hbm, ig_ref),
        (k_hbm, k_ref),
        (v_hbm, v_ref),
        (q_hbm, q_ref),
        (gate_hbm.at[0], gate_ref.at[mt]),
        (og_hbm, og_ref),
        (hgain_hbm, hgain_ref),
        (ngain_hbm, ngain_ref),
        (routes_hbm, routes_ref),
        (group_hbm, group_ref),
        (scores_hbm, scores_ref),
        (res_hbm, res_ref),
        (up_hbm.at[0], up_ref.at[mt]),
        (wo_hbm, wo_ref),
    ]
    for start, size, ref in zip(starts, WIDTHS, down_refs):
        loads.append((down_hbm.at[0, :, pl.ds(start, size)], ref.at[mt]))
    loads = [
        pltpu.make_async_copy(source, target, load_sem.at[n])
        for n, (source, target) in enumerate(loads)
    ]
    for load in loads[:6]:
        load.start()

    for step in range(1, PLANE):
        peer = zed * PLANE + lax.rem(place + step, PLANE)
        pl.semaphore_signal(barrier, inc=1, device_id={"sp": peer}, device_id_type=MESH)
    for step in range(1, planes):
        peer = lax.rem(zed + step, planes) * PLANE + place
        pl.semaphore_signal(barrier, inc=1, device_id={"sp": peer}, device_id_type=MESH)
    for step in range(1, tp_count):
        peer = lax.rem(mt + step, tp_count)
        pl.semaphore_signal(barrier, inc=1, device_id={"tp": peer}, device_id_type=MESH)

    gate_ring, up_ring, *down_rings = [
        Ring(ref, item, mt, tp_count, ring_send, ring_recv)
        for item, ref in enumerate((gate_ref, up_ref, *down_refs))
    ]
    for load in loads[:5]:
        load.wait()

    small = jnp.exp(-fg_ref[...])
    series = small * (1.0 - small * (0.5 - small * (1.0 / 3.0 - 0.25 * small)))
    log_forget = -jnp.where(small < 0.01, series, jnp.log(1.0 + small))
    cum = running(log_forget, jnp.add, 0.0)
    level_in = ig_ref[...] - cum
    peak = running(level_in, jnp.maximum, VERY_NEGATIVE)
    total_col = cum[:, length - 1 : length]
    top_col = peak[:, length - 1 : length]
    weight = jnp.exp(level_in - top_col)

    lane_head = lax.broadcasted_iota(jnp.int32, (1, width), 1) // head
    masks = [lane_head == h for h in range(head_count)]

    def spread(column):
        row = jnp.zeros((1, width), F32)
        for h in range(head_count):
            row = jnp.where(masks[h], column[h : h + 1, :], row)
        return row

    total_row = spread(total_col)
    level_row = total_row + spread(top_col)

    k_turned = k_ref[...].astype(F32).T
    parts = [
        k_turned[h * head : (h + 1) * head, :] * weight[h : h + 1, :] for h in range(head_count)
    ]
    high, low = halves(jnp.concatenate(parts, axis=0))
    values = v_ref[...]
    whole = dot(high, values) + dot(low, values)
    memory = jnp.zeros((head, width), F32)
    for h in range(head_count):
        memory = jnp.where(masks[h], whole[h * head : (h + 1) * head, :], memory)
    rows = head // PLANE
    for n in range(PLANE):
        put(s1_ref, n, (total_row, level_row, memory[n * rows : (n + 1) * rows, :]))
    put(r1_ref, place, unpacked(s1_ref, place))

    pl.semaphore_wait(barrier, PLANE + planes + tp_count - 3)
    loads[5].wait()

    def whole(source, landed, send_sem, recv_sem):
        return pltpu.make_async_remote_copy(
            src_ref=source,
            dst_ref=landed,
            send_sem=send_sem,
            recv_sem=recv_sem,
            device_id={"tp": lax.rem(mt + 1, tp_count)},
            device_id_type=MESH,
        )

    def exchange1(step):
        peer = lax.rem(place + step, PLANE)
        return pltpu.make_async_remote_copy(
            src_ref=s1_ref.at[peer],
            dst_ref=r1_ref.at[place],
            send_sem=send1,
            recv_sem=recv1,
            device_id={"sp": zed * PLANE + peer},
            device_id_type=MESH,
        )

    def exchange2(step):
        peer = lax.rem(zed + step, planes)
        return pltpu.make_async_remote_copy(
            src_ref=s2_ref.at[0],
            dst_ref=r2_ref.at[zed],
            send_sem=send2,
            recv_sem=recv2,
            device_id={"sp": peer * PLANE + place},
            device_id_type=MESH,
        )

    def exchange3(step):
        peer = lax.rem(place + step, PLANE)
        return pltpu.make_async_remote_copy(
            src_ref=s3_ref.at[peer],
            dst_ref=r3_ref.at[place],
            send_sem=send3,
            recv_sem=recv3,
            device_id={"sp": zed * PLANE + peer},
            device_id_type=MESH,
        )

    rest = pl.ds(0, PLANE - 1)
    rest_planes = pl.ds(0, planes - 1)
    for step in range(1, PLANE):
        exchange1(step).start()
    gate_ring.start()
    for load in loads[6:]:
        load.start()

    peak_cols = jnp.concatenate([peak, jnp.zeros((8 - head_count, length), F32)], axis=0).T
    peak_wide = jnp.zeros((length, width), F32)
    for h in range(head_count):
        peak_wide = jnp.where(masks[h], peak_cols[:, h : h + 1], peak_wide)
    peak_ref[...] = peak_wide
    scale = head**-0.5
    block = 128

    def inner(t):
        span = (t + 1) * block
        rows_t = slice(t * block, span)
        query = q_ref[rows_t, :].astype(F32) * scale
        position = lax.broadcasted_iota(jnp.int32, (block, span), 0) + t * block
        source = lax.broadcasted_iota(jnp.int32, (block, span), 1)
        causal = source <= position
        found = jnp.zeros((block, width), F32)
        for h in range(head_count):
            mine = jnp.where(masks[h], query, 0.0).astype(BF16)
            scores = dot_t(mine, k_ref[0:span, :])
            gap = level_in[h : h + 1, 0:span] - peak_cols[rows_t, h : h + 1]
            pairs = scores * jnp.exp(jnp.where(causal, gap, VERY_NEGATIVE))
            pairs_high, pairs_low = halves(pairs)
            part = dot(pairs_high, v_ref[0:span, :]) + dot(pairs_low, v_ref[0:span, :])
            found = jnp.where(masks[h], part, found)
        intra_ref[rows_t, :] = found

    inner(0)
    inner(1)

    whole(s1_ref.at[rest], r1_ref.at[rest], send1, recv1).wait()
    identity = (
        jnp.zeros((1, width), F32),
        jnp.full((1, width), VERY_NEGATIVE, F32),
        jnp.zeros((rows, width), F32),
    )
    prior = [identity]
    for n in range(PLANE):
        prior.append(join(prior[-1], unpacked(r1_ref, n)))
    put(s2_ref, 0, prior[-1])
    put(r2_ref, zed, prior[-1])
    for step in range(1, planes):
        exchange2(step).start()

    inner(2)

    whole(r2_ref.at[rest_planes], r2_ref.at[rest_planes], send2, recv2).wait()
    entering = identity
    for n in range(planes):
        later = join(entering, unpacked(r2_ref, n))
        entering = tuple(jnp.where(n < zed, new, old) for new, old in zip(later, entering))
    for n in range(PLANE):
        put(s3_ref, n, join(entering, prior[n]))
    put(r3_ref, place, unpacked(s3_ref, place))
    for step in range(1, PLANE):
        exchange3(step).start()

    inner(3)

    whole(s3_ref.at[rest], r3_ref.at[rest], send3, recv3).wait()
    prior_total = r3_ref[0, 8:9, :]
    prior_level = r3_ref[0, 9:10, :]
    start_level = jnp.maximum(prior_level, prior_total)
    opening = jnp.exp(prior_level - start_level)
    began = jnp.concatenate([r3_ref[n, 0:8, :] for n in range(PLANE)], axis=0) * opening
    blocks = jnp.concatenate([jnp.where(masks[h], began, 0.0) for h in range(head_count)], axis=0)
    block_high, block_low = halves(blocks)
    row_head = lax.broadcasted_iota(jnp.int32, (width, width), 0) // head
    column_head = lax.broadcasted_iota(jnp.int32, (width, width), 1) // head
    averaging = jnp.where(row_head == column_head, 1.0 / head, 0.0).astype(BF16)
    for load in loads[6:]:
        load.wait()
    gain = jnp.concatenate([hgain_ref[h : h + 1, :] for h in range(head_count)], axis=1)

    def exchange4(step):
        peer = lax.rem(mt + step, tp_count)
        return pltpu.make_async_remote_copy(
            src_ref=mix_ref.at[peer],
            dst_ref=mrecv_ref.at[mt],
            send_sem=send4,
            recv_sem=recv4,
            device_id={"tp": peer},
            device_id_type=MESH,
        )

    for step in (2, 1, 3, 0):
        peer = lax.rem(mt + step, tp_count)
        rows_t = pl.ds(pl.multiple_of(peer * tokens, tokens), tokens)
        queries = (q_ref[rows_t, :].astype(F32) * scale).astype(BF16)
        carried = dot(queries, block_high) + dot(queries, block_low)
        peak_wide = peak_ref[rows_t, :]
        level = jnp.maximum(peak_wide, start_level)
        cell = jnp.exp(peak_wide - level) * intra_ref[rows_t, :]
        cell = cell + jnp.exp(start_level - level) * carried
        square_high, square_low = halves(cell * cell)
        mean = dot(square_high, averaging) + dot(square_low, averaging)
        gate = 1.0 / (1.0 + jnp.exp(-og_ref[rows_t, :].astype(F32)))
        mixed = (gate * (cell * lax.rsqrt(mean + EPSILON) * gain)).astype(BF16)
        if step:
            mix_ref[peer] = mixed
            exchange4(step).start()
        else:
            mrecv_ref[mt] = mixed
    up_ring.start()

    routes = routes_ref[:, pl.ds(pl.multiple_of(mt * tokens, tokens), tokens)]
    first, second = slots_of(routes, capacity, sp_count)
    slot = lax.broadcasted_iota(jnp.int32, (slots, tokens), 0)
    select = jnp.where((slot == first) | (slot == second), 1.0, 0.0).astype(BF16)

    others = pl.ds(0, tp_count - 1)
    whole(mix_ref.at[others], mrecv_ref.at[others], send4, recv4).wait()
    gathered = jnp.concatenate([mrecv_ref[n] for n in range(tp_count)], axis=1)
    piece = 512
    squares = jnp.zeros((tokens, 1), F32)
    for n in range(model // piece):
        cols = slice(n * piece, (n + 1) * piece)
        projected = dot(gathered, wo_ref[:, cols])
        stream = (res_ref[:, cols].astype(F32) + projected).astype(BF16)
        stream_ref[:, cols] = stream
        stream = stream.astype(F32)
        squares = squares + jnp.sum(stream * stream, axis=1, keepdims=True)
    inverse = lax.rsqrt(squares * (1.0 / model) + EPSILON)
    for n in range(model // piece):
        cols = slice(n * piece, (n + 1) * piece)
        normed = (stream_ref[:, cols].astype(F32) * inverse * ngain_ref[:, cols]).astype(BF16)
        chosen = dot(select, normed).reshape(sp_count, capacity, piece)
        send_ref[:, :, cols] = chosen.astype(BF16)

    arrived_ref[0] = send_ref[me]
    row_parts = 2
    group = sp_count // row_parts

    def dispatch(step):
        peer = ring_peer(me, step, sp_count)
        return pltpu.make_async_remote_copy(
            src_ref=send_ref.at[peer],
            dst_ref=arrived_ref.at[step],
            send_sem=send5,
            recv_sem=recv5.at[step // group],
            device_id={"sp": peer},
            device_id_type=MESH,
        )

    def go(step, _):
        dispatch(step).start()
        return 0

    lax.fori_loop(1, sp_count, go, 0)
    gate_ring.forward()

    own = pl.ds(pl.multiple_of(mt * tokens, tokens), tokens)
    scores = scores_ref[:, own]
    most = jnp.maximum(scores[0:1, :], scores[1:2, :])
    first_exp = jnp.exp(scores[0:1, :] - most)
    second_exp = jnp.exp(scores[1:2, :] - most)
    share = group_ref[:, own] / (first_exp + second_exp)
    weights = jnp.where(slot == first, share * first_exp, 0.0)
    weights = jnp.where(slot == second, share * second_exp, weights).T
    weights_high, weights_low = halves(weights)

    up_ring.forward()
    down_rings[0].start()
    down_rings[1].start()

    many = slots // row_parts
    rows_in = arrived_ref.reshape(slots, model)

    def expert(part, quarter):
        rows_t = slice(part * many, (part + 1) * many)
        gated = dot(rows_in[rows_t, :], gate_ref[quarter])
        raised = dot(rows_in[rows_t, :], up_ref[quarter])
        hidden_ref[quarter, rows_t, :] = (gated / (1.0 + jnp.exp(-gated)) * raised).astype(BF16)

    for part in range(row_parts):
        landed = arrived_ref.at[pl.ds(part * group, group - (part == 0))]
        whole(landed, landed, send5, recv5.at[part]).wait_recv()

        def near(n, _):
            expert(part, lax.rem(mt + n + tp_count - 1, tp_count))
            return 0

        lax.fori_loop(0, 3, near, 0)
    gate_ring.complete()
    up_ring.complete()
    for part in range(row_parts):
        expert(part, lax.rem(mt + 2, tp_count))

    wide = 256

    def give(chunk, step):
        peer = ring_source(me, step, sp_count)
        return pltpu.make_async_remote_copy(
            src_ref=back_refs[chunk].at[step],
            dst_ref=answer_refs[chunk].at[me],
            send_sem=send6.at[chunk],
            recv_sem=recv6.at[chunk],
            device_id={"sp": peer},
            device_id_type=MESH,
        )

    def answer(chunk):
        down_ref, back_ref = down_refs[chunk], back_refs[chunk]
        for n in range(WIDTHS[chunk] // wide):
            cols = slice(n * wide, (n + 1) * wide)
            result = jnp.zeros((slots, wide), F32)
            for quarter in range(tp_count):
                result = result + dot(hidden_ref[quarter], down_ref[quarter, :, cols])
            back_ref[:, :, cols] = result.reshape(sp_count, capacity, wide).astype(BF16)
        answer_refs[chunk][me] = back_ref[0]

        def go(step, _):
            give(chunk, step).start()
            return 0

        lax.fori_loop(1, sp_count, go, 0)

    def finish(chunk):
        back, landed = back_refs[chunk], answer_refs[chunk]
        most_of = pl.ds(0, sp_count - 1)
        whole(back.at[most_of], landed.at[most_of], send6.at[chunk], recv6.at[chunk]).wait()
        answers = answer_refs[chunk].reshape(slots, WIDTHS[chunk])[...]
        mix = dot(weights_high, answers) + dot(weights_low, answers)
        cols = slice(starts[chunk], starts[chunk] + WIDTHS[chunk])
        out_ref[:, cols] = (stream_ref[:, cols].astype(F32) + mix).astype(BF16)

    for chunk in range(chunks):
        down_rings[chunk].forward()
        if chunk + 2 < chunks:
            down_rings[chunk + 2].start()
        down_rings[chunk].complete()
        answer(chunk)
    for chunk in range(chunks):
        finish(chunk)
    left = send_ref.at[pl.ds(0, sp_count - 1)]
    whole(left, left, send5, recv5.at[0]).wait_send()
    for ring in (gate_ring, up_ring, *down_rings):
        ring.sent()


def shards(
    residual,
    queries,
    key_vectors,
    value_vectors,
    output_gate,
    input_gate,
    forget_gate,
    head_gain,
    output_weight,
    norm_gain,
    route_experts,
    group_weight,
    expert_scores,
    gate_weight,
    up_weight,
    down_weight,
):
    sp_count = lax.axis_size("sp")
    tp_count = lax.axis_size("tp")
    length, width = queries.shape
    head_count, head = input_gate.shape[1], head_gain.shape[1]
    tokens, model = residual.shape
    capacity = 4 * tokens // sp_count
    hidden_part = gate_weight.shape[2]
    planes = sp_count // PLANE
    slots = sp_count * capacity
    dma = pltpu.SemaphoreType.DMA
    vmem = pltpu.VMEM
    return pl.pallas_call(
        functools.partial(layer_kernel, sp_count, tp_count, head_count),
        out_shape=jax.ShapeDtypeStruct((tokens, model), BF16),
        in_specs=[pl.BlockSpec(memory_space=pl.ANY)] * 16,
        out_specs=pl.BlockSpec(memory_space=pltpu.VMEM),
        scratch_shapes=[
            vmem((length, width), BF16),
            vmem((length, width), BF16),
            vmem((length, width), BF16),
            vmem((length, width), BF16),
            vmem((head_count, length), F32),
            vmem((head_count, length), F32),
            vmem((head_count, head), F32),
            vmem(output_weight.shape, BF16),
            vmem((tokens, model), BF16),
            vmem((1, model), F32),
            vmem((2, length), jnp.int32),
            vmem((1, length), F32),
            vmem((2, length), F32),
            vmem((tp_count, model, hidden_part), BF16),
            vmem((tp_count, model, hidden_part), BF16),
            vmem((length, width), F32),
            vmem((length, width), F32),
            vmem((PLANE, 16, width), F32),
            vmem((PLANE, 16, width), F32),
            vmem((1, 16, width), F32),
            vmem((planes, 16, width), F32),
            vmem((PLANE, 16, width), F32),
            vmem((PLANE, 16, width), F32),
            vmem((tp_count, tokens, width), BF16),
            vmem((tp_count, tokens, width), BF16),
            vmem((tokens, model), BF16),
            vmem((sp_count, capacity, model), BF16),
            vmem((sp_count, capacity, model), BF16),
            vmem((tp_count, slots, hidden_part), BF16),
            dma((15 + len(WIDTHS),)),
            dma,
            dma,
            dma,
            dma,
            dma,
            dma,
            dma,
            dma,
            dma,
            dma((2,)),
            dma((len(WIDTHS),)),
            dma((len(WIDTHS),)),
            dma((2 + len(WIDTHS), 4)),
            dma((2 + len(WIDTHS), 4)),
            *[vmem((sp_count, capacity, n), BF16) for n in WIDTHS],
            *[vmem((sp_count, capacity, n), BF16) for n in WIDTHS],
            *[vmem((tp_count, hidden_part, n), BF16) for n in WIDTHS],
        ],
        compiler_params=pltpu.CompilerParams(
            collective_id=0, has_side_effects=True, vmem_limit_bytes=66_000_000
        ),
    )(
        queries,
        key_vectors,
        value_vectors,
        output_gate,
        input_gate.T,
        forget_gate.T,
        head_gain,
        output_weight,
        residual,
        norm_gain.reshape(1, model),
        route_experts.T,
        group_weight.reshape(1, length),
        expert_scores.T,
        gate_weight,
        up_weight,
        down_weight,
    )


def solution(mesh):
    both = ("sp", "tp")
    return jax.shard_map(
        shards,
        mesh=mesh,
        in_specs=(
            P(both, None),
            P("sp", "tp"),
            P("sp", "tp"),
            P("sp", "tp"),
            P("sp", "tp"),
            P("sp", "tp"),
            P("sp", "tp"),
            P("tp", None),
            P(),
            P(),
            P("sp", None),
            P("sp"),
            P("sp", None),
            P("sp", None, "tp"),
            P("sp", None, "tp"),
            P("sp", "tp", None),
        ),
        out_specs=P(both, None),
        check_vma=False,
    )
```

```python
import functools

import jax
import jax.numpy as jnp
from jax import lax
from jax.experimental import pallas as pl
from jax.experimental.pallas import tpu as pltpu
from jax.sharding import PartitionSpec as P

EPSILON = 1e-06
VERY_NEGATIVE = -1e30
MESH = pl.DeviceIdType.MESH
PLANE = 8
WIDTHS = (256, 256, 256, 256, 512, 512)
F32 = jnp.float32
BF16 = jnp.bfloat16


def dot(a, b):
    return jnp.dot(a, b, preferred_element_type=F32)


def dot_t(a, b):
    return lax.dot_general(a, b, (((1,), (1,)), ((), ())), preferred_element_type=F32)


def halves(x):
    high = x.astype(BF16)
    return high, (x - high.astype(F32)).astype(BF16)


def shifted(x, by, fill):
    lane = lax.broadcasted_iota(jnp.int32, x.shape, 1)
    return jnp.where(lane >= by, pltpu.roll(x, by, 1), fill)


def running(x, combine, fill):
    by = 1
    while by < x.shape[1]:
        x = combine(x, shifted(x, by, fill))
        by *= 2
    return x


def join(early, late):
    early_total, early_level, early_memory = early
    late_total, late_level, late_memory = late
    level = jnp.maximum(late_total + early_level, late_level)
    memory = (
        jnp.exp(late_total + early_level - level) * early_memory
        + jnp.exp(late_level - level) * late_memory
    )
    return early_total + late_total, level, memory


def unpacked(memory_ref, scalars_ref, index):
    scalars = scalars_ref[index]
    return scalars[0:1, :], scalars[1:2, :], memory_ref[index]


def put(memory_ref, scalars_ref, index, state):
    total, level, memory = state
    memory_ref[index] = memory
    scalars_ref[index, 0:1, :] = total
    scalars_ref[index, 1:2, :] = level


def ring_peer(me, step, count):
    away = (step + 1) // 2
    sign = 2 * lax.rem(step, 2) - 1
    return lax.rem(me + sign * away + count, count)


def ring_source(me, step, count):
    away = (step + 1) // 2
    sign = 2 * lax.rem(step, 2) - 1
    return lax.rem(me - sign * away + count, count)


def slots_of(routes, capacity, experts):
    tokens = routes.shape[1]
    expert = lax.broadcasted_iota(jnp.int32, (experts, tokens), 0)
    first = expert == routes[0:1, :]
    second = expert == routes[1:2, :]
    row = lax.broadcasted_iota(jnp.int32, (tokens, tokens), 0)
    column = lax.broadcasted_iota(jnp.int32, (tokens, tokens), 1)
    earlier = jnp.where(row < column, 1.0, 0.0).astype(BF16)
    ones = jnp.ones((tokens, tokens), BF16)
    first_hot = jnp.where(first, 1.0, 0.0).astype(BF16)
    second_hot = jnp.where(second, 1.0, 0.0).astype(BF16)
    first_rank = dot(first_hot, earlier)
    second_rank = dot(first_hot, ones) + dot(second_hot, earlier)
    places = []
    for hot, rank, route in ((first, first_rank, routes[0:1, :]), (second, second_rank, routes[1:2, :])):
        own = jnp.sum(jnp.where(hot, rank, 0.0), axis=0, keepdims=True)
        places.append(route * capacity + own.astype(jnp.int32))
    return places


class Ring:
    def __init__(self, ref, item, me, count, sends, arrivals):
        self.ref, self.item, self.me, self.count = ref, item, me, count
        self.sends, self.arrivals = sends, arrivals
        self.half = ref.shape[1] // 2

    def copy(self, kind):
        right = lax.rem(self.me + 1, self.count)
        left = lax.rem(self.me + self.count - 1, self.count)
        first, last = pl.ds(0, self.half), pl.ds(self.half, self.half)
        source, target = (
            (self.ref.at[self.me], right),
            (self.ref.at[self.me], left),
            (self.ref.at[left, first], right),
            (self.ref.at[right, last], left),
        )[kind]
        return pltpu.make_async_remote_copy(
            src_ref=source,
            dst_ref=source,
            send_sem=self.sends.at[self.item, kind],
            recv_sem=self.arrivals.at[self.item, kind],
            device_id={"tp": target},
            device_id_type=MESH,
        )

    def arrival(self, kind):
        right = lax.rem(self.me + 1, self.count)
        left = lax.rem(self.me + self.count - 1, self.count)
        across = lax.rem(self.me + 2, self.count)
        first, last = pl.ds(0, self.half), pl.ds(self.half, self.half)
        source, landed = (
            (self.ref.at[self.me], self.ref.at[left]),
            (self.ref.at[self.me], self.ref.at[right]),
            (self.ref.at[left, first], self.ref.at[across, first]),
            (self.ref.at[right, last], self.ref.at[across, last]),
        )[kind]
        return pltpu.make_async_remote_copy(
            src_ref=source,
            dst_ref=landed,
            send_sem=self.sends.at[self.item, kind],
            recv_sem=self.arrivals.at[self.item, kind],
            device_id={"tp": right},
            device_id_type=MESH,
        )

    def start(self):
        self.copy(0).start()
        self.copy(1).start()

    def forward(self):
        self.arrival(0).wait_recv()
        self.copy(2).start()
        self.arrival(1).wait_recv()
        self.copy(3).start()

    def complete(self):
        self.arrival(2).wait_recv()
        self.arrival(3).wait_recv()

    def sent(self):
        for kind in range(4):
            self.copy(kind).wait_send()


def layer_kernel(sp_count, tp_count, head_count, *refs):
    chunks = len(WIDTHS)
    starts = [sum(WIDTHS[:n]) for n in range(chunks)]
    listed = refs[len(refs) - 3 * chunks :]
    refs = refs[: len(refs) - 3 * chunks]
    back_refs, answer_refs = listed[:chunks], listed[chunks : 2 * chunks]
    down_refs = listed[2 * chunks :]
    (
        q_hbm,
        k_hbm,
        v_hbm,
        og_hbm,
        ig_hbm,
        fg_hbm,
        hgain_hbm,
        wo_hbm,
        res_hbm,
        ngain_hbm,
        routes_hbm,
        group_hbm,
        scores_hbm,
        gate_hbm,
        up_hbm,
        down_hbm,
        out_ref,
        q_ref,
        k_ref,
        v_ref,
        og_ref,
        ig_ref,
        fg_ref,
        hgain_ref,
        wo_ref,
        res_ref,
        ngain_ref,
        routes_ref,
        group_ref,
        scores_ref,
        gate_ref,
        up_ref,
        intra_ref,
        peak_ref,
        s1_ref,
        s1s_ref,
        r1_ref,
        r1s_ref,
        s2_ref,
        s2s_ref,
        r2_ref,
        r2s_ref,
        s3_ref,
        r3_ref,
        mix_ref,
        mrecv_ref,
        stream_ref,
        send_ref,
        arrived_ref,
        hidden_ref,
        load_sem,
        send1,
        recv1,
        send1s,
        recv1s,
        send2,
        recv2,
        send2s,
        recv2s,
        send3,
        recv3,
        send4,
        recv4,
        send5,
        recv5,
        send6,
        recv6,
        ring_send,
        ring_recv,
    ) = refs
    me = lax.axis_index("sp")
    mt = lax.axis_index("tp")
    zed = me // PLANE
    place = lax.rem(me, PLANE)
    planes = sp_count // PLANE
    length, width = q_ref.shape
    head = width // head_count
    tokens = length // tp_count
    capacity = send_ref.shape[1]
    model = send_ref.shape[2]
    slots = sp_count * capacity

    barrier = pltpu.get_barrier_semaphore()

    loads = [
        (fg_hbm, fg_ref),
        (ig_hbm, ig_ref),
        (k_hbm, k_ref),
        (v_hbm, v_ref),
        (q_hbm, q_ref),
        (gate_hbm.at[0], gate_ref.at[mt]),
        (og_hbm, og_ref),
        (hgain_hbm, hgain_ref),
        (ngain_hbm, ngain_ref),
        (routes_hbm, routes_ref),
        (group_hbm, group_ref),
        (scores_hbm, scores_ref),
        (res_hbm, res_ref),
        (up_hbm.at[0], up_ref.at[mt]),
        (wo_hbm, wo_ref),
    ]
    for start, size, ref in zip(starts, WIDTHS, down_refs):
        loads.append((down_hbm.at[0, :, pl.ds(start, size)], ref.at[mt]))
    loads = [
        pltpu.make_async_copy(source, target, load_sem.at[n])
        for n, (source, target) in enumerate(loads)
    ]
    for load in loads[:6]:
        load.start()

    for step in range(1, PLANE):
        peer = zed * PLANE + lax.rem(place + step, PLANE)
        pl.semaphore_signal(barrier, inc=1, device_id={"sp": peer}, device_id_type=MESH)
    for step in range(1, planes):
        peer = lax.rem(zed + step, planes) * PLANE + place
        pl.semaphore_signal(barrier, inc=1, device_id={"sp": peer}, device_id_type=MESH)
    for step in range(1, tp_count):
        peer = lax.rem(mt + step, tp_count)
        pl.semaphore_signal(barrier, inc=1, device_id={"tp": peer}, device_id_type=MESH)

    early = 3 * model // 4
    gate_first = gate_ref.at[:, pl.ds(0, early), :]
    gate_last = gate_ref.at[:, pl.ds(early, model - early), :]
    gate_ring, gate_rest, up_ring, *down_rings = [
        Ring(ref, item, mt, tp_count, ring_send, ring_recv)
        for item, ref in enumerate((gate_first, gate_last, up_ref, *down_refs))
    ]
    for load in loads[:5]:
        load.wait()

    small = jnp.exp(-fg_ref[...])
    series = small * (1.0 - small * (0.5 - small * (1.0 / 3.0 - 0.25 * small)))
    log_forget = -jnp.where(small < 0.01, series, jnp.log(1.0 + small))
    cum = running(log_forget, jnp.add, 0.0)
    level_in = ig_ref[...] - cum
    peak = running(level_in, jnp.maximum, VERY_NEGATIVE)
    total_col = cum[:, length - 1 : length]
    top_col = peak[:, length - 1 : length]
    weight = jnp.exp(level_in - top_col)

    lane_head = lax.broadcasted_iota(jnp.int32, (1, width), 1) // head
    masks = [lane_head == h for h in range(head_count)]

    def spread(column):
        row = jnp.zeros((1, width), F32)
        for h in range(head_count):
            row = jnp.where(masks[h], column[h : h + 1, :], row)
        return row

    total_row = spread(total_col)
    level_row = total_row + spread(top_col)

    k_turned = k_ref[...].astype(F32).T
    parts = [
        k_turned[h * head : (h + 1) * head, :] * weight[h : h + 1, :] for h in range(head_count)
    ]
    high, low = halves(jnp.concatenate(parts, axis=0))
    values = v_ref[...]
    whole = dot(high, values) + dot(low, values)
    memory = jnp.zeros((head, width), F32)
    for h in range(head_count):
        memory = jnp.where(masks[h], whole[h * head : (h + 1) * head, :], memory)
    rows = head // PLANE
    for n in range(PLANE):
        s1_ref[n] = memory[n * rows : (n + 1) * rows, :]
    s1s_ref[0, 0:1, :] = total_row
    s1s_ref[0, 1:2, :] = level_row
    r1_ref[place] = s1_ref[place]
    r1s_ref[place] = s1s_ref[0]

    pl.semaphore_wait(barrier, PLANE + planes + tp_count - 3)
    loads[5].wait()

    def whole(source, landed, send_sem, recv_sem):
        return pltpu.make_async_remote_copy(
            src_ref=source,
            dst_ref=landed,
            send_sem=send_sem,
            recv_sem=recv_sem,
            device_id={"tp": lax.rem(mt + 1, tp_count)},
            device_id_type=MESH,
        )

    def exchange1(step):
        peer = lax.rem(place + step, PLANE)
        return pltpu.make_async_remote_copy(
            src_ref=s1_ref.at[peer],
            dst_ref=r1_ref.at[place],
            send_sem=send1,
            recv_sem=recv1,
            device_id={"sp": zed * PLANE + peer},
            device_id_type=MESH,
        )

    def exchange1s(step):
        peer = lax.rem(place + step, PLANE)
        return pltpu.make_async_remote_copy(
            src_ref=s1s_ref.at[0],
            dst_ref=r1s_ref.at[place],
            send_sem=send1s,
            recv_sem=recv1s,
            device_id={"sp": zed * PLANE + peer},
            device_id_type=MESH,
        )

    def exchange2s(step):
        peer = lax.rem(zed + step, planes)
        return pltpu.make_async_remote_copy(
            src_ref=s2s_ref.at[0],
            dst_ref=r2s_ref.at[zed],
            send_sem=send2s,
            recv_sem=recv2s,
            device_id={"sp": peer * PLANE + place},
            device_id_type=MESH,
        )

    def exchange2(step):
        peer = lax.rem(zed + step, planes)
        return pltpu.make_async_remote_copy(
            src_ref=s2_ref.at[0],
            dst_ref=r2_ref.at[zed],
            send_sem=send2,
            recv_sem=recv2,
            device_id={"sp": peer * PLANE + place},
            device_id_type=MESH,
        )

    def exchange3(step):
        peer = lax.rem(place + step, PLANE)
        return pltpu.make_async_remote_copy(
            src_ref=s3_ref.at[peer],
            dst_ref=r3_ref.at[place],
            send_sem=send3,
            recv_sem=recv3,
            device_id={"sp": zed * PLANE + peer},
            device_id_type=MESH,
        )

    rest = pl.ds(0, PLANE - 1)
    rest_planes = pl.ds(0, planes - 1)
    for step in range(1, PLANE):
        exchange1s(step).start()
        exchange1(step).start()
    gate_ring.start()
    for load in loads[6:]:
        load.start()

    peak_cols = jnp.concatenate([peak, jnp.zeros((8 - head_count, length), F32)], axis=0).T
    peak_wide = jnp.zeros((length, width), F32)
    for h in range(head_count):
        peak_wide = jnp.where(masks[h], peak_cols[:, h : h + 1], peak_wide)
    peak_ref[...] = peak_wide
    scale = head**-0.5
    block = 128

    def inner(t):
        span = (t + 1) * block
        rows_t = slice(t * block, span)
        query = q_ref[rows_t, :].astype(F32) * scale
        position = lax.broadcasted_iota(jnp.int32, (block, span), 0) + t * block
        source = lax.broadcasted_iota(jnp.int32, (block, span), 1)
        causal = source <= position
        found = jnp.zeros((block, width), F32)
        for h in range(head_count):
            mine = jnp.where(masks[h], query, 0.0).astype(BF16)
            scores = dot_t(mine, k_ref[0:span, :])
            gap = level_in[h : h + 1, 0:span] - peak_cols[rows_t, h : h + 1]
            pairs = scores * jnp.exp(jnp.where(causal, gap, VERY_NEGATIVE))
            pairs_high, pairs_low = halves(pairs)
            part = dot(pairs_high, v_ref[0:span, :]) + dot(pairs_low, v_ref[0:span, :])
            found = jnp.where(masks[h], part, found)
        intra_ref[rows_t, :] = found

    inner(0)
    inner(1)

    whole(r1s_ref.at[rest], r1s_ref.at[rest], send1s, recv1s).wait()
    whole(r1_ref.at[rest], r1_ref.at[rest], send1, recv1).wait()
    identity = (
        jnp.zeros((1, width), F32),
        jnp.full((1, width), VERY_NEGATIVE, F32),
        jnp.zeros((rows, width), F32),
    )
    prior = [identity]
    for n in range(PLANE):
        prior.append(join(prior[-1], unpacked(r1_ref, r1s_ref, n)))
    put(s2_ref, s2s_ref, 0, prior[-1])
    put(r2_ref, r2s_ref, zed, prior[-1])
    for step in range(1, planes):
        exchange2s(step).start()
        exchange2(step).start()

    inner(2)

    whole(r2s_ref.at[rest_planes], r2s_ref.at[rest_planes], send2s, recv2s).wait()
    whole(r2_ref.at[rest_planes], r2_ref.at[rest_planes], send2, recv2).wait()
    entering = identity
    for n in range(planes):
        later = join(entering, unpacked(r2_ref, r2s_ref, n))
        entering = tuple(jnp.where(n < zed, new, old) for new, old in zip(later, entering))
    prior_total, prior_level, _ = identity
    for n in range(PLANE):
        total, level, part = join(entering, prior[n])
        s3_ref[n] = part
        prior_total = jnp.where(place == n, total, prior_total)
        prior_level = jnp.where(place == n, level, prior_level)
    r3_ref[place] = s3_ref[place]
    for step in range(1, PLANE):
        exchange3(step).start()

    inner(3)

    whole(s3_ref.at[rest], r3_ref.at[rest], send3, recv3).wait()
    start_level = jnp.maximum(prior_level, prior_total)
    opening = jnp.exp(prior_level - start_level)
    began = jnp.concatenate([r3_ref[n] for n in range(PLANE)], axis=0) * opening
    blocks = jnp.concatenate([jnp.where(masks[h], began, 0.0) for h in range(head_count)], axis=0)
    block_high, block_low = halves(blocks)
    row_head = lax.broadcasted_iota(jnp.int32, (width, width), 0) // head
    column_head = lax.broadcasted_iota(jnp.int32, (width, width), 1) // head
    averaging = jnp.where(row_head == column_head, 1.0 / head, 0.0).astype(BF16)
    for load in loads[6:]:
        load.wait()
    gain = jnp.concatenate([hgain_ref[h : h + 1, :] for h in range(head_count)], axis=1)

    def exchange4(step):
        peer = lax.rem(mt + step, tp_count)
        return pltpu.make_async_remote_copy(
            src_ref=mix_ref.at[peer],
            dst_ref=mrecv_ref.at[mt],
            send_sem=send4,
            recv_sem=recv4,
            device_id={"tp": peer},
            device_id_type=MESH,
        )

    for step in (2, 1, 3, 0):
        peer = lax.rem(mt + step, tp_count)
        rows_t = pl.ds(pl.multiple_of(peer * tokens, tokens), tokens)
        queries = (q_ref[rows_t, :].astype(F32) * scale).astype(BF16)
        carried = dot(queries, block_high) + dot(queries, block_low)
        peak_wide = peak_ref[rows_t, :]
        level = jnp.maximum(peak_wide, start_level)
        cell = jnp.exp(peak_wide - level) * intra_ref[rows_t, :]
        cell = cell + jnp.exp(start_level - level) * carried
        square_high, square_low = halves(cell * cell)
        mean = dot(square_high, averaging) + dot(square_low, averaging)
        gate = 1.0 / (1.0 + jnp.exp(-og_ref[rows_t, :].astype(F32)))
        mixed = (gate * (cell * lax.rsqrt(mean + EPSILON) * gain)).astype(BF16)
        if step:
            mix_ref[peer] = mixed
            exchange4(step).start()
        else:
            mrecv_ref[mt] = mixed
    gate_rest.start()
    up_ring.start()

    routes = routes_ref[:, pl.ds(pl.multiple_of(mt * tokens, tokens), tokens)]
    first, second = slots_of(routes, capacity, sp_count)
    slot = lax.broadcasted_iota(jnp.int32, (slots, tokens), 0)
    select = jnp.where((slot == first) | (slot == second), 1.0, 0.0).astype(BF16)

    others = pl.ds(0, tp_count - 1)
    whole(mix_ref.at[others], mrecv_ref.at[others], send4, recv4).wait()
    gathered = jnp.concatenate([mrecv_ref[n] for n in range(tp_count)], axis=1)
    piece = 512
    squares = jnp.zeros((tokens, 1), F32)
    for n in range(model // piece):
        cols = slice(n * piece, (n + 1) * piece)
        projected = dot(gathered, wo_ref[:, cols])
        stream = (res_ref[:, cols].astype(F32) + projected).astype(BF16)
        stream_ref[:, cols] = stream
        stream = stream.astype(F32)
        squares = squares + jnp.sum(stream * stream, axis=1, keepdims=True)
    inverse = lax.rsqrt(squares * (1.0 / model) + EPSILON)
    for n in range(model // piece):
        cols = slice(n * piece, (n + 1) * piece)
        normed = (stream_ref[:, cols].astype(F32) * inverse * ngain_ref[:, cols]).astype(BF16)
        chosen = dot(select, normed).reshape(sp_count, capacity, piece)
        send_ref[:, :, cols] = chosen.astype(BF16)

    arrived_ref[0] = send_ref[me]
    row_parts = 2
    group = sp_count // row_parts

    def dispatch(step):
        peer = ring_peer(me, step, sp_count)
        return pltpu.make_async_remote_copy(
            src_ref=send_ref.at[peer],
            dst_ref=arrived_ref.at[step],
            send_sem=send5,
            recv_sem=recv5.at[step // group],
            device_id={"sp": peer},
            device_id_type=MESH,
        )

    def go(step, _):
        dispatch(step).start()
        return 0

    lax.fori_loop(1, sp_count, go, 0)
    gate_ring.forward()
    gate_rest.forward()
    down_rings[0].start()

    own = pl.ds(pl.multiple_of(mt * tokens, tokens), tokens)
    scores = scores_ref[:, own]
    most = jnp.maximum(scores[0:1, :], scores[1:2, :])
    first_exp = jnp.exp(scores[0:1, :] - most)
    second_exp = jnp.exp(scores[1:2, :] - most)
    share = group_ref[:, own] / (first_exp + second_exp)
    weights = jnp.where(slot == first, share * first_exp, 0.0)
    weights = jnp.where(slot == second, share * second_exp, weights).T
    weights_high, weights_low = halves(weights)

    up_ring.forward()

    many = slots // row_parts
    rows_in = arrived_ref.reshape(slots, model)

    def expert(part, quarter):
        rows_t = slice(part * many, (part + 1) * many)
        gated = dot(rows_in[rows_t, :], gate_ref[quarter])
        raised = dot(rows_in[rows_t, :], up_ref[quarter])
        hidden_ref[quarter, rows_t, :] = (gated / (1.0 + jnp.exp(-gated)) * raised).astype(BF16)

    for part in range(row_parts):
        landed = arrived_ref.at[pl.ds(part * group, group - (part == 0))]
        whole(landed, landed, send5, recv5.at[part]).wait_recv()

        def near(n, _):
            expert(part, lax.rem(mt + n + tp_count - 1, tp_count))
            return 0

        lax.fori_loop(0, 3, near, 0)
        if part == 0:
            down_rings[0].forward()
            down_rings[1].start()
            down_rings[2].start()
    gate_ring.complete()
    gate_rest.complete()
    up_ring.complete()
    for part in range(row_parts):
        expert(part, lax.rem(mt + 2, tp_count))

    wide = 256

    def give(chunk, step):
        peer = ring_source(me, step, sp_count)
        return pltpu.make_async_remote_copy(
            src_ref=back_refs[chunk].at[step],
            dst_ref=answer_refs[chunk].at[me],
            send_sem=send6.at[chunk],
            recv_sem=recv6.at[chunk],
            device_id={"sp": peer},
            device_id_type=MESH,
        )

    def answer(chunk):
        down_ref, back_ref = down_refs[chunk], back_refs[chunk]
        for n in range(WIDTHS[chunk] // wide):
            cols = slice(n * wide, (n + 1) * wide)
            result = jnp.zeros((slots, wide), F32)
            for quarter in range(tp_count):
                result = result + dot(hidden_ref[quarter], down_ref[quarter, :, cols])
            back_ref[:, :, cols] = result.reshape(sp_count, capacity, wide).astype(BF16)
        answer_refs[chunk][me] = back_ref[0]

        def go(step, _):
            give(chunk, step).start()
            return 0

        lax.fori_loop(1, sp_count, go, 0)

    def finish(chunk):
        back, landed = back_refs[chunk], answer_refs[chunk]
        most_of = pl.ds(0, sp_count - 1)
        whole(back.at[most_of], landed.at[most_of], send6.at[chunk], recv6.at[chunk]).wait()
        answers = answer_refs[chunk].reshape(slots, WIDTHS[chunk])[...]
        mix = dot(weights_high, answers) + dot(weights_low, answers)
        cols = slice(starts[chunk], starts[chunk] + WIDTHS[chunk])
        out_ref[:, cols] = (stream_ref[:, cols].astype(F32) + mix).astype(BF16)

    for chunk in range(chunks):
        if chunk:
            down_rings[chunk].forward()
            if chunk + 2 < chunks:
                down_rings[chunk + 2].start()
        down_rings[chunk].complete()
        answer(chunk)
    for chunk in range(chunks):
        finish(chunk)
    left = send_ref.at[pl.ds(0, sp_count - 1)]
    whole(left, left, send5, recv5.at[0]).wait_send()
    for ring in (gate_ring, gate_rest, up_ring, *down_rings):
        ring.sent()


def shards(
    residual,
    queries,
    key_vectors,
    value_vectors,
    output_gate,
    input_gate,
    forget_gate,
    head_gain,
    output_weight,
    norm_gain,
    route_experts,
    group_weight,
    expert_scores,
    gate_weight,
    up_weight,
    down_weight,
):
    sp_count = lax.axis_size("sp")
    tp_count = lax.axis_size("tp")
    length, width = queries.shape
    head_count, head = input_gate.shape[1], head_gain.shape[1]
    tokens, model = residual.shape
    capacity = 4 * tokens // sp_count
    hidden_part = gate_weight.shape[2]
    planes = sp_count // PLANE
    slots = sp_count * capacity
    rows = head // PLANE
    dma = pltpu.SemaphoreType.DMA
    vmem = pltpu.VMEM
    return pl.pallas_call(
        functools.partial(layer_kernel, sp_count, tp_count, head_count),
        out_shape=jax.ShapeDtypeStruct((tokens, model), BF16),
        in_specs=[pl.BlockSpec(memory_space=pl.ANY)] * 16,
        out_specs=pl.BlockSpec(memory_space=pltpu.VMEM),
        scratch_shapes=[
            vmem((length, width), BF16),
            vmem((length, width), BF16),
            vmem((length, width), BF16),
            vmem((length, width), BF16),
            vmem((head_count, length), F32),
            vmem((head_count, length), F32),
            vmem((head_count, head), F32),
            vmem(output_weight.shape, BF16),
            vmem((tokens, model), BF16),
            vmem((1, model), F32),
            vmem((2, length), jnp.int32),
            vmem((1, length), F32),
            vmem((2, length), F32),
            vmem((tp_count, model, hidden_part), BF16),
            vmem((tp_count, model, hidden_part), BF16),
            vmem((length, width), F32),
            vmem((length, width), F32),
            vmem((PLANE, rows, width), F32),
            vmem((1, 2, width), F32),
            vmem((PLANE, rows, width), F32),
            vmem((PLANE, 2, width), F32),
            vmem((1, rows, width), F32),
            vmem((1, 2, width), F32),
            vmem((planes, rows, width), F32),
            vmem((planes, 2, width), F32),
            vmem((PLANE, rows, width), F32),
            vmem((PLANE, rows, width), F32),
            vmem((tp_count, tokens, width), BF16),
            vmem((tp_count, tokens, width), BF16),
            vmem((tokens, model), BF16),
            vmem((sp_count, capacity, model), BF16),
            vmem((sp_count, capacity, model), BF16),
            vmem((tp_count, slots, hidden_part), BF16),
            dma((15 + len(WIDTHS),)),
            dma,
            dma,
            dma,
            dma,
            dma,
            dma,
            dma,
            dma,
            dma,
            dma,
            dma,
            dma,
            dma,
            dma((2,)),
            dma((len(WIDTHS),)),
            dma((len(WIDTHS),)),
            dma((3 + len(WIDTHS), 4)),
            dma((3 + len(WIDTHS), 4)),
            *[vmem((sp_count, capacity, n), BF16) for n in WIDTHS],
            *[vmem((sp_count, capacity, n), BF16) for n in WIDTHS],
            *[vmem((tp_count, hidden_part, n), BF16) for n in WIDTHS],
        ],
        compiler_params=pltpu.CompilerParams(
            collective_id=0, has_side_effects=True, vmem_limit_bytes=66_000_000
        ),
    )(
        queries,
        key_vectors,
        value_vectors,
        output_gate,
        input_gate.T,
        forget_gate.T,
        head_gain,
        output_weight,
        residual,
        norm_gain.reshape(1, model),
        route_experts.T,
        group_weight.reshape(1, length),
        expert_scores.T,
        gate_weight,
        up_weight,
        down_weight,
    )


def solution(mesh):
    both = ("sp", "tp")
    return jax.shard_map(
        shards,
        mesh=mesh,
        in_specs=(
            P(both, None),
            P("sp", "tp"),
            P("sp", "tp"),
            P("sp", "tp"),
            P("sp", "tp"),
            P("sp", "tp"),
            P("sp", "tp"),
            P("tp", None),
            P(),
            P(),
            P("sp", None),
            P("sp"),
            P("sp", None),
            P("sp", None, "tp"),
            P("sp", None, "tp"),
            P("sp", "tp", None),
        ),
        out_specs=P(both, None),
        check_vma=False,
    )
```

```python
import functools

import jax
import jax.numpy as jnp
from jax import lax
from jax.experimental import pallas as pl
from jax.experimental.pallas import tpu as pltpu
from jax.sharding import PartitionSpec as P

EPSILON = 1e-06
VERY_NEGATIVE = -1e30
MESH = pl.DeviceIdType.MESH
PLANE = 8
WIDTHS = (256, 256, 256, 256, 512, 512)
F32 = jnp.float32
BF16 = jnp.bfloat16


def dot(a, b):
    return jnp.dot(a, b, preferred_element_type=F32)


def dot_t(a, b):
    return lax.dot_general(a, b, (((1,), (1,)), ((), ())), preferred_element_type=F32)


def halves(x):
    high = x.astype(BF16)
    return high, (x - high.astype(F32)).astype(BF16)


def shifted(x, by, fill):
    lane = lax.broadcasted_iota(jnp.int32, x.shape, 1)
    return jnp.where(lane >= by, pltpu.roll(x, by, 1), fill)


def running(x, combine, fill):
    by = 1
    while by < x.shape[1]:
        x = combine(x, shifted(x, by, fill))
        by *= 2
    return x


def join(early, late):
    early_total, early_level, early_memory = early
    late_total, late_level, late_memory = late
    level = jnp.maximum(late_total + early_level, late_level)
    memory = (
        jnp.exp(late_total + early_level - level) * early_memory
        + jnp.exp(late_level - level) * late_memory
    )
    return early_total + late_total, level, memory


def unpacked(memory_ref, scalars_ref, index):
    scalars = scalars_ref[index]
    return scalars[0:1, :], scalars[1:2, :], memory_ref[index]


def put(memory_ref, scalars_ref, index, state):
    total, level, memory = state
    memory_ref[index] = memory
    scalars_ref[index, 0:1, :] = total
    scalars_ref[index, 1:2, :] = level


def ring_peer(me, step, count):
    away = (step + 1) // 2
    sign = 2 * lax.rem(step, 2) - 1
    return lax.rem(me + sign * away + count, count)


def ring_source(me, step, count):
    away = (step + 1) // 2
    sign = 2 * lax.rem(step, 2) - 1
    return lax.rem(me - sign * away + count, count)


def slots_of(routes, capacity, experts):
    tokens = routes.shape[1]
    expert = lax.broadcasted_iota(jnp.int32, (experts, tokens), 0)
    first = expert == routes[0:1, :]
    second = expert == routes[1:2, :]
    row = lax.broadcasted_iota(jnp.int32, (tokens, tokens), 0)
    column = lax.broadcasted_iota(jnp.int32, (tokens, tokens), 1)
    earlier = jnp.where(row < column, 1.0, 0.0).astype(BF16)
    ones = jnp.ones((tokens, tokens), BF16)
    first_hot = jnp.where(first, 1.0, 0.0).astype(BF16)
    second_hot = jnp.where(second, 1.0, 0.0).astype(BF16)
    first_rank = dot(first_hot, earlier)
    second_rank = dot(first_hot, ones) + dot(second_hot, earlier)
    places = []
    for hot, rank, route in ((first, first_rank, routes[0:1, :]), (second, second_rank, routes[1:2, :])):
        own = jnp.sum(jnp.where(hot, rank, 0.0), axis=0, keepdims=True)
        places.append(route * capacity + own.astype(jnp.int32))
    return places


class Ring:
    def __init__(self, ref, item, me, count, sends, arrivals):
        self.ref, self.item, self.me, self.count = ref, item, me, count
        self.sends, self.arrivals = sends, arrivals
        self.half = ref.shape[1] // 2

    def copy(self, kind):
        right = lax.rem(self.me + 1, self.count)
        left = lax.rem(self.me + self.count - 1, self.count)
        first, last = pl.ds(0, self.half), pl.ds(self.half, self.half)
        source, target = (
            (self.ref.at[self.me], right),
            (self.ref.at[self.me], left),
            (self.ref.at[left, first], right),
            (self.ref.at[right, last], left),
        )[kind]
        return pltpu.make_async_remote_copy(
            src_ref=source,
            dst_ref=source,
            send_sem=self.sends.at[self.item, kind],
            recv_sem=self.arrivals.at[self.item, kind],
            device_id={"tp": target},
            device_id_type=MESH,
        )

    def arrival(self, kind):
        right = lax.rem(self.me + 1, self.count)
        left = lax.rem(self.me + self.count - 1, self.count)
        across = lax.rem(self.me + 2, self.count)
        first, last = pl.ds(0, self.half), pl.ds(self.half, self.half)
        source, landed = (
            (self.ref.at[self.me], self.ref.at[left]),
            (self.ref.at[self.me], self.ref.at[right]),
            (self.ref.at[left, first], self.ref.at[across, first]),
            (self.ref.at[right, last], self.ref.at[across, last]),
        )[kind]
        return pltpu.make_async_remote_copy(
            src_ref=source,
            dst_ref=landed,
            send_sem=self.sends.at[self.item, kind],
            recv_sem=self.arrivals.at[self.item, kind],
            device_id={"tp": right},
            device_id_type=MESH,
        )

    def start(self):
        self.copy(0).start()
        self.copy(1).start()

    def forward(self):
        self.arrival(0).wait_recv()
        self.copy(2).start()
        self.arrival(1).wait_recv()
        self.copy(3).start()

    def complete(self):
        self.arrival(2).wait_recv()
        self.arrival(3).wait_recv()

    def sent(self):
        for kind in range(4):
            self.copy(kind).wait_send()


def layer_kernel(sp_count, tp_count, head_count, *refs):
    chunks = len(WIDTHS)
    starts = [sum(WIDTHS[:n]) for n in range(chunks)]
    listed = refs[len(refs) - 3 * chunks :]
    refs = refs[: len(refs) - 3 * chunks]
    back_refs, answer_refs = listed[:chunks], listed[chunks : 2 * chunks]
    down_refs = listed[2 * chunks :]
    (
        q_hbm,
        k_hbm,
        v_hbm,
        og_hbm,
        ig_hbm,
        fg_hbm,
        hgain_hbm,
        wo_hbm,
        res_hbm,
        ngain_hbm,
        routes_hbm,
        group_hbm,
        scores_hbm,
        gate_hbm,
        up_hbm,
        down_hbm,
        out_ref,
        q_ref,
        k_ref,
        v_ref,
        og_ref,
        ig_ref,
        fg_ref,
        hgain_ref,
        wo_ref,
        res_ref,
        ngain_ref,
        routes_ref,
        group_ref,
        scores_ref,
        gate_ref,
        up_ref,
        intra_ref,
        peak_ref,
        s1_ref,
        s1s_ref,
        r1_ref,
        r1s_ref,
        s2_ref,
        s2s_ref,
        r2_ref,
        r2s_ref,
        s3_ref,
        r3_ref,
        mix_ref,
        mrecv_ref,
        stream_ref,
        send_ref,
        arrived_ref,
        hidden_ref,
        load_sem,
        send1,
        recv1,
        send1s,
        recv1s,
        send2,
        recv2,
        send2s,
        recv2s,
        send3,
        recv3,
        send4,
        recv4,
        send5,
        recv5,
        send6,
        recv6,
        ring_send,
        ring_recv,
    ) = refs
    me = lax.axis_index("sp")
    mt = lax.axis_index("tp")
    zed = me // PLANE
    place = lax.rem(me, PLANE)
    planes = sp_count // PLANE
    length, width = q_ref.shape
    head = width // head_count
    tokens = length // tp_count
    capacity = send_ref.shape[1]
    model = send_ref.shape[2]
    slots = sp_count * capacity

    barrier = pltpu.get_barrier_semaphore()

    loads = [
        (fg_hbm, fg_ref),
        (ig_hbm, ig_ref),
        (k_hbm, k_ref),
        (v_hbm, v_ref),
        (q_hbm, q_ref),
        (gate_hbm.at[0], gate_ref.at[mt]),
        (og_hbm, og_ref),
        (hgain_hbm, hgain_ref),
        (ngain_hbm, ngain_ref),
        (routes_hbm, routes_ref),
        (group_hbm, group_ref),
        (scores_hbm, scores_ref),
        (res_hbm, res_ref),
        (up_hbm.at[0], up_ref.at[mt]),
        (wo_hbm, wo_ref),
    ]
    for start, size, ref in zip(starts, WIDTHS, down_refs):
        loads.append((down_hbm.at[0, :, pl.ds(start, size)], ref.at[mt]))
    loads = [
        pltpu.make_async_copy(source, target, load_sem.at[n])
        for n, (source, target) in enumerate(loads)
    ]
    for load in loads[:6]:
        load.start()

    for step in range(1, PLANE):
        peer = zed * PLANE + lax.rem(place + step, PLANE)
        pl.semaphore_signal(barrier, inc=1, device_id={"sp": peer}, device_id_type=MESH)
    for step in range(1, planes):
        peer = lax.rem(zed + step, planes) * PLANE + place
        pl.semaphore_signal(barrier, inc=1, device_id={"sp": peer}, device_id_type=MESH)
    for step in range(1, tp_count):
        peer = lax.rem(mt + step, tp_count)
        pl.semaphore_signal(barrier, inc=1, device_id={"tp": peer}, device_id_type=MESH)

    early = 3 * model // 4
    gate_first = gate_ref.at[:, pl.ds(0, early), :]
    gate_last = gate_ref.at[:, pl.ds(early, model - early), :]
    gate_ring, gate_rest, up_ring, *down_rings = [
        Ring(ref, item, mt, tp_count, ring_send, ring_recv)
        for item, ref in enumerate((gate_first, gate_last, up_ref, *down_refs))
    ]
    for load in loads[:5]:
        load.wait()

    small = jnp.exp(-fg_ref[...])
    series = small * (1.0 - small * (0.5 - small * (1.0 / 3.0 - 0.25 * small)))
    log_forget = -jnp.where(small < 0.01, series, jnp.log(1.0 + small))
    cum = running(log_forget, jnp.add, 0.0)
    level_in = ig_ref[...] - cum
    peak = running(level_in, jnp.maximum, VERY_NEGATIVE)
    total_col = cum[:, length - 1 : length]
    top_col = peak[:, length - 1 : length]
    weight = jnp.exp(level_in - top_col)

    lane_head = lax.broadcasted_iota(jnp.int32, (1, width), 1) // head
    masks = [lane_head == h for h in range(head_count)]

    def spread(column):
        row = jnp.zeros((1, width), F32)
        for h in range(head_count):
            row = jnp.where(masks[h], column[h : h + 1, :], row)
        return row

    total_row = spread(total_col)
    level_row = total_row + spread(top_col)

    k_turned = k_ref[...].astype(F32).T
    parts = [
        k_turned[h * head : (h + 1) * head, :] * weight[h : h + 1, :] for h in range(head_count)
    ]
    high, low = halves(jnp.concatenate(parts, axis=0))
    values = v_ref[...]
    whole = dot(high, values) + dot(low, values)
    memory = jnp.zeros((head, width), F32)
    for h in range(head_count):
        memory = jnp.where(masks[h], whole[h * head : (h + 1) * head, :], memory)
    rows = head // PLANE
    for n in range(PLANE):
        s1_ref[n] = memory[n * rows : (n + 1) * rows, :]
    s1s_ref[0, 0:1, :] = total_row
    s1s_ref[0, 1:2, :] = level_row
    r1_ref[place] = s1_ref[place]
    r1s_ref[place] = s1s_ref[0]

    pl.semaphore_wait(barrier, PLANE + planes + tp_count - 3)
    loads[5].wait()

    def whole(source, landed, send_sem, recv_sem):
        return pltpu.make_async_remote_copy(
            src_ref=source,
            dst_ref=landed,
            send_sem=send_sem,
            recv_sem=recv_sem,
            device_id={"tp": lax.rem(mt + 1, tp_count)},
            device_id_type=MESH,
        )

    def exchange1(step):
        peer = lax.rem(place + step, PLANE)
        return pltpu.make_async_remote_copy(
            src_ref=s1_ref.at[peer],
            dst_ref=r1_ref.at[place],
            send_sem=send1,
            recv_sem=recv1,
            device_id={"sp": zed * PLANE + peer},
            device_id_type=MESH,
        )

    def exchange1s(step):
        peer = lax.rem(place + step, PLANE)
        return pltpu.make_async_remote_copy(
            src_ref=s1s_ref.at[0],
            dst_ref=r1s_ref.at[place],
            send_sem=send1s,
            recv_sem=recv1s,
            device_id={"sp": zed * PLANE + peer},
            device_id_type=MESH,
        )

    def exchange2s(step):
        peer = lax.rem(zed + step, planes)
        return pltpu.make_async_remote_copy(
            src_ref=s2s_ref.at[0],
            dst_ref=r2s_ref.at[zed],
            send_sem=send2s,
            recv_sem=recv2s,
            device_id={"sp": peer * PLANE + place},
            device_id_type=MESH,
        )

    def exchange2(step):
        peer = lax.rem(zed + step, planes)
        return pltpu.make_async_remote_copy(
            src_ref=s2_ref.at[0],
            dst_ref=r2_ref.at[zed],
            send_sem=send2,
            recv_sem=recv2,
            device_id={"sp": peer * PLANE + place},
            device_id_type=MESH,
        )

    def exchange3(step):
        peer = lax.rem(place + step, PLANE)
        return pltpu.make_async_remote_copy(
            src_ref=s3_ref.at[peer],
            dst_ref=r3_ref.at[place],
            send_sem=send3,
            recv_sem=recv3,
            device_id={"sp": zed * PLANE + peer},
            device_id_type=MESH,
        )

    rest = pl.ds(0, PLANE - 1)
    rest_planes = pl.ds(0, planes - 1)
    for step in range(1, PLANE):
        exchange1s(step).start()
        exchange1(step).start()
    gate_ring.start()
    for load in loads[6:]:
        load.start()

    peak_cols = jnp.concatenate([peak, jnp.zeros((8 - head_count, length), F32)], axis=0).T
    peak_wide = jnp.zeros((length, width), F32)
    for h in range(head_count):
        peak_wide = jnp.where(masks[h], peak_cols[:, h : h + 1], peak_wide)
    peak_ref[...] = peak_wide
    scale = head**-0.5
    block = 128

    def inner(t):
        span = (t + 1) * block
        rows_t = slice(t * block, span)
        query = q_ref[rows_t, :].astype(F32) * scale
        position = lax.broadcasted_iota(jnp.int32, (block, span), 0) + t * block
        source = lax.broadcasted_iota(jnp.int32, (block, span), 1)
        causal = source <= position
        found = jnp.zeros((block, width), F32)
        for h in range(head_count):
            mine = jnp.where(masks[h], query, 0.0).astype(BF16)
            scores = dot_t(mine, k_ref[0:span, :])
            gap = level_in[h : h + 1, 0:span] - peak_cols[rows_t, h : h + 1]
            pairs = scores * jnp.exp(jnp.where(causal, gap, VERY_NEGATIVE))
            pairs_high, pairs_low = halves(pairs)
            part = dot(pairs_high, v_ref[0:span, :]) + dot(pairs_low, v_ref[0:span, :])
            found = jnp.where(masks[h], part, found)
        intra_ref[rows_t, :] = found

    inner(0)
    inner(1)

    whole(r1s_ref.at[rest], r1s_ref.at[rest], send1s, recv1s).wait()
    whole(r1_ref.at[rest], r1_ref.at[rest], send1, recv1).wait()
    identity = (
        jnp.zeros((1, width), F32),
        jnp.full((1, width), VERY_NEGATIVE, F32),
        jnp.zeros((rows, width), F32),
    )
    prior = [identity]
    for n in range(PLANE):
        prior.append(join(prior[-1], unpacked(r1_ref, r1s_ref, n)))
    put(s2_ref, s2s_ref, 0, prior[-1])
    put(r2_ref, r2s_ref, zed, prior[-1])
    for step in range(1, planes):
        exchange2s(step).start()
        exchange2(step).start()

    inner(2)

    whole(r2s_ref.at[rest_planes], r2s_ref.at[rest_planes], send2s, recv2s).wait()
    whole(r2_ref.at[rest_planes], r2_ref.at[rest_planes], send2, recv2).wait()
    entering = identity
    for n in range(planes):
        later = join(entering, unpacked(r2_ref, r2s_ref, n))
        entering = tuple(jnp.where(n < zed, new, old) for new, old in zip(later, entering))
    prior_total, prior_level, _ = identity
    for n in range(PLANE):
        total, level, part = join(entering, prior[n])
        s3_ref[n] = part
        prior_total = jnp.where(place == n, total, prior_total)
        prior_level = jnp.where(place == n, level, prior_level)
    r3_ref[place] = s3_ref[place]
    for step in range(1, PLANE):
        exchange3(step).start()

    inner(3)

    whole(s3_ref.at[rest], r3_ref.at[rest], send3, recv3).wait()
    start_level = jnp.maximum(prior_level, prior_total)
    opening = jnp.exp(prior_level - start_level)
    began = jnp.concatenate([r3_ref[n] for n in range(PLANE)], axis=0) * opening
    blocks = jnp.concatenate([jnp.where(masks[h], began, 0.0) for h in range(head_count)], axis=0)
    block_high, block_low = halves(blocks)
    row_head = lax.broadcasted_iota(jnp.int32, (width, width), 0) // head
    column_head = lax.broadcasted_iota(jnp.int32, (width, width), 1) // head
    averaging = jnp.where(row_head == column_head, 1.0 / head, 0.0).astype(BF16)
    for load in loads[6:]:
        load.wait()
    gain = jnp.concatenate([hgain_ref[h : h + 1, :] for h in range(head_count)], axis=1)

    def exchange4(step):
        peer = lax.rem(mt + step, tp_count)
        return pltpu.make_async_remote_copy(
            src_ref=mix_ref.at[peer],
            dst_ref=mrecv_ref.at[mt],
            send_sem=send4,
            recv_sem=recv4,
            device_id={"tp": peer},
            device_id_type=MESH,
        )

    for step in (2, 1, 3, 0):
        peer = lax.rem(mt + step, tp_count)
        rows_t = pl.ds(pl.multiple_of(peer * tokens, tokens), tokens)
        queries = (q_ref[rows_t, :].astype(F32) * scale).astype(BF16)
        carried = dot(queries, block_high) + dot(queries, block_low)
        peak_wide = peak_ref[rows_t, :]
        level = jnp.maximum(peak_wide, start_level)
        cell = jnp.exp(peak_wide - level) * intra_ref[rows_t, :]
        cell = cell + jnp.exp(start_level - level) * carried
        square_high, square_low = halves(cell * cell)
        mean = dot(square_high, averaging) + dot(square_low, averaging)
        gate = 1.0 / (1.0 + jnp.exp(-og_ref[rows_t, :].astype(F32)))
        mixed = (gate * (cell * lax.rsqrt(mean + EPSILON) * gain)).astype(BF16)
        if step:
            mix_ref[peer] = mixed
            exchange4(step).start()
        else:
            mrecv_ref[mt] = mixed
    gate_rest.start()
    up_ring.start()

    routes = routes_ref[:, pl.ds(pl.multiple_of(mt * tokens, tokens), tokens)]
    first, second = slots_of(routes, capacity, sp_count)
    slot = lax.broadcasted_iota(jnp.int32, (slots, tokens), 0)
    select = jnp.where((slot == first) | (slot == second), 1.0, 0.0).astype(BF16)

    others = pl.ds(0, tp_count - 1)
    whole(mix_ref.at[others], mrecv_ref.at[others], send4, recv4).wait()
    gathered = jnp.concatenate([mrecv_ref[n] for n in range(tp_count)], axis=1)
    piece = 512
    squares = jnp.zeros((tokens, 1), F32)
    for n in range(model // piece):
        cols = slice(n * piece, (n + 1) * piece)
        projected = dot(gathered, wo_ref[:, cols])
        stream = (res_ref[:, cols].astype(F32) + projected).astype(BF16)
        stream_ref[:, cols] = stream
        stream = stream.astype(F32)
        squares = squares + jnp.sum(stream * stream, axis=1, keepdims=True)
    inverse = lax.rsqrt(squares * (1.0 / model) + EPSILON)
    for n in range(model // piece):
        cols = slice(n * piece, (n + 1) * piece)
        normed = (stream_ref[:, cols].astype(F32) * inverse * ngain_ref[:, cols]).astype(BF16)
        chosen = dot(select, normed).reshape(sp_count, capacity, piece)
        send_ref[:, :, cols] = chosen.astype(BF16)

    arrived_ref[0] = send_ref[me]
    row_parts = 2
    group = sp_count // row_parts

    def dispatch(step):
        peer = ring_peer(me, step, sp_count)
        return pltpu.make_async_remote_copy(
            src_ref=send_ref.at[peer],
            dst_ref=arrived_ref.at[step],
            send_sem=send5,
            recv_sem=recv5.at[step // group],
            device_id={"sp": peer},
            device_id_type=MESH,
        )

    def go(step, _):
        dispatch(step).start()
        return 0

    lax.fori_loop(1, sp_count, go, 0)
    gate_ring.forward()
    gate_rest.forward()
    down_rings[0].start()

    own = pl.ds(pl.multiple_of(mt * tokens, tokens), tokens)
    scores = scores_ref[:, own]
    most = jnp.maximum(scores[0:1, :], scores[1:2, :])
    first_exp = jnp.exp(scores[0:1, :] - most)
    second_exp = jnp.exp(scores[1:2, :] - most)
    share = group_ref[:, own] / (first_exp + second_exp)
    weights = jnp.where(slot == first, share * first_exp, 0.0)
    weights = jnp.where(slot == second, share * second_exp, weights).T
    weights_high, weights_low = halves(weights)

    up_ring.forward()

    many = slots // row_parts
    rows_in = arrived_ref.reshape(slots, model)

    def expert(part, quarter):
        rows_t = slice(part * many, (part + 1) * many)
        gated = dot(rows_in[rows_t, :], gate_ref[quarter])
        raised = dot(rows_in[rows_t, :], up_ref[quarter])
        hidden_ref[quarter, rows_t, :] = (gated / (1.0 + jnp.exp(-gated)) * raised).astype(BF16)

    for part in range(row_parts):
        landed = arrived_ref.at[pl.ds(part * group, group - (part == 0))]
        whole(landed, landed, send5, recv5.at[part]).wait_recv()

        def near(n, _):
            expert(part, lax.rem(mt + n + tp_count - 1, tp_count))
            return 0

        lax.fori_loop(0, 3, near, 0)
        if part == 0:
            down_rings[0].forward()
            down_rings[1].start()
    gate_ring.complete()
    gate_rest.complete()
    up_ring.complete()
    for part in range(row_parts):
        expert(part, lax.rem(mt + 2, tp_count))

    wide = 256

    def give(chunk, step):
        peer = ring_source(me, step, sp_count)
        return pltpu.make_async_remote_copy(
            src_ref=back_refs[chunk].at[step],
            dst_ref=answer_refs[chunk].at[me],
            send_sem=send6.at[chunk],
            recv_sem=recv6.at[chunk],
            device_id={"sp": peer},
            device_id_type=MESH,
        )

    def answer(chunk):
        down_ref, back_ref = down_refs[chunk], back_refs[chunk]
        for n in range(WIDTHS[chunk] // wide):
            cols = slice(n * wide, (n + 1) * wide)
            result = jnp.zeros((slots, wide), F32)
            for quarter in range(tp_count):
                result = result + dot(hidden_ref[quarter], down_ref[quarter, :, cols])
            back_ref[:, :, cols] = result.reshape(sp_count, capacity, wide).astype(BF16)
        answer_refs[chunk][me] = back_ref[0]

        def go(step, _):
            give(chunk, step).start()
            return 0

        lax.fori_loop(1, sp_count, go, 0)

    def finish(chunk):
        back, landed = back_refs[chunk], answer_refs[chunk]
        most_of = pl.ds(0, sp_count - 1)
        whole(back.at[most_of], landed.at[most_of], send6.at[chunk], recv6.at[chunk]).wait()
        answers = answer_refs[chunk].reshape(slots, WIDTHS[chunk])[...]
        mix = dot(weights_high, answers) + dot(weights_low, answers)
        cols = slice(starts[chunk], starts[chunk] + WIDTHS[chunk])
        out_ref[:, cols] = (stream_ref[:, cols].astype(F32) + mix).astype(BF16)

    for chunk in range(chunks):
        if chunk:
            down_rings[chunk].forward()
            if chunk + 1 < chunks:
                down_rings[chunk + 1].start()
        down_rings[chunk].complete()
        answer(chunk)
    for chunk in range(chunks):
        finish(chunk)
    left = send_ref.at[pl.ds(0, sp_count - 1)]
    whole(left, left, send5, recv5.at[0]).wait_send()
    for ring in (gate_ring, gate_rest, up_ring, *down_rings):
        ring.sent()


def shards(
    residual,
    queries,
    key_vectors,
    value_vectors,
    output_gate,
    input_gate,
    forget_gate,
    head_gain,
    output_weight,
    norm_gain,
    route_experts,
    group_weight,
    expert_scores,
    gate_weight,
    up_weight,
    down_weight,
):
    sp_count = lax.axis_size("sp")
    tp_count = lax.axis_size("tp")
    length, width = queries.shape
    head_count, head = input_gate.shape[1], head_gain.shape[1]
    tokens, model = residual.shape
    capacity = 4 * tokens // sp_count
    hidden_part = gate_weight.shape[2]
    planes = sp_count // PLANE
    slots = sp_count * capacity
    rows = head // PLANE
    dma = pltpu.SemaphoreType.DMA
    vmem = pltpu.VMEM
    return pl.pallas_call(
        functools.partial(layer_kernel, sp_count, tp_count, head_count),
        out_shape=jax.ShapeDtypeStruct((tokens, model), BF16),
        in_specs=[pl.BlockSpec(memory_space=pl.ANY)] * 16,
        out_specs=pl.BlockSpec(memory_space=pltpu.VMEM),
        scratch_shapes=[
            vmem((length, width), BF16),
            vmem((length, width), BF16),
            vmem((length, width), BF16),
            vmem((length, width), BF16),
            vmem((head_count, length), F32),
            vmem((head_count, length), F32),
            vmem((head_count, head), F32),
            vmem(output_weight.shape, BF16),
            vmem((tokens, model), BF16),
            vmem((1, model), F32),
            vmem((2, length), jnp.int32),
            vmem((1, length), F32),
            vmem((2, length), F32),
            vmem((tp_count, model, hidden_part), BF16),
            vmem((tp_count, model, hidden_part), BF16),
            vmem((length, width), F32),
            vmem((length, width), F32),
            vmem((PLANE, rows, width), F32),
            vmem((1, 2, width), F32),
            vmem((PLANE, rows, width), F32),
            vmem((PLANE, 2, width), F32),
            vmem((1, rows, width), F32),
            vmem((1, 2, width), F32),
            vmem((planes, rows, width), F32),
            vmem((planes, 2, width), F32),
            vmem((PLANE, rows, width), F32),
            vmem((PLANE, rows, width), F32),
            vmem((tp_count, tokens, width), BF16),
            vmem((tp_count, tokens, width), BF16),
            vmem((tokens, model), BF16),
            vmem((sp_count, capacity, model), BF16),
            vmem((sp_count, capacity, model), BF16),
            vmem((tp_count, slots, hidden_part), BF16),
            dma((15 + len(WIDTHS),)),
            dma,
            dma,
            dma,
            dma,
            dma,
            dma,
            dma,
            dma,
            dma,
            dma,
            dma,
            dma,
            dma,
            dma((2,)),
            dma((len(WIDTHS),)),
            dma((len(WIDTHS),)),
            dma((3 + len(WIDTHS), 4)),
            dma((3 + len(WIDTHS), 4)),
            *[vmem((sp_count, capacity, n), BF16) for n in WIDTHS],
            *[vmem((sp_count, capacity, n), BF16) for n in WIDTHS],
            *[vmem((tp_count, hidden_part, n), BF16) for n in WIDTHS],
        ],
        compiler_params=pltpu.CompilerParams(
            collective_id=0, has_side_effects=True, vmem_limit_bytes=66_000_000
        ),
    )(
        queries,
        key_vectors,
        value_vectors,
        output_gate,
        input_gate.T,
        forget_gate.T,
        head_gain,
        output_weight,
        residual,
        norm_gain.reshape(1, model),
        route_experts.T,
        group_weight.reshape(1, length),
        expert_scores.T,
        gate_weight,
        up_weight,
        down_weight,
    )


def solution(mesh):
    both = ("sp", "tp")
    return jax.shard_map(
        shards,
        mesh=mesh,
        in_specs=(
            P(both, None),
            P("sp", "tp"),
            P("sp", "tp"),
            P("sp", "tp"),
            P("sp", "tp"),
            P("sp", "tp"),
            P("sp", "tp"),
            P("tp", None),
            P(),
            P(),
            P("sp", None),
            P("sp"),
            P("sp", None),
            P("sp", None, "tp"),
            P("sp", None, "tp"),
            P("sp", "tp", None),
        ),
        out_specs=P(both, None),
        check_vma=False,
    )
```

```python
import functools

import jax
import jax.numpy as jnp
from jax import lax
from jax.experimental import pallas as pl
from jax.experimental.pallas import tpu as pltpu
from jax.sharding import PartitionSpec as P

EPSILON = 1e-06
VERY_NEGATIVE = -1e30
MESH = pl.DeviceIdType.MESH
PLANE = 8
WIDTHS = (256, 256, 384, 384, 384, 384)
F32 = jnp.float32
BF16 = jnp.bfloat16


def dot(a, b):
    return jnp.dot(a, b, preferred_element_type=F32)


def dot_t(a, b):
    return lax.dot_general(a, b, (((1,), (1,)), ((), ())), preferred_element_type=F32)


def halves(x):
    high = x.astype(BF16)
    return high, (x - high.astype(F32)).astype(BF16)


def shifted(x, by, fill):
    lane = lax.broadcasted_iota(jnp.int32, x.shape, 1)
    return jnp.where(lane >= by, pltpu.roll(x, by, 1), fill)


def running(x, combine, fill):
    by = 1
    while by < x.shape[1]:
        x = combine(x, shifted(x, by, fill))
        by *= 2
    return x


def join(early, late):
    early_total, early_level, early_memory = early
    late_total, late_level, late_memory = late
    level = jnp.maximum(late_total + early_level, late_level)
    memory = (
        jnp.exp(late_total + early_level - level) * early_memory
        + jnp.exp(late_level - level) * late_memory
    )
    return early_total + late_total, level, memory


def unpacked(memory_ref, scalars_ref, index):
    scalars = scalars_ref[index]
    return scalars[0:1, :], scalars[1:2, :], memory_ref[index]


def put(memory_ref, scalars_ref, index, state):
    total, level, memory = state
    memory_ref[index] = memory
    scalars_ref[index, 0:1, :] = total
    scalars_ref[index, 1:2, :] = level


def ring_peer(me, step, count):
    away = (step + 1) // 2
    sign = 2 * lax.rem(step, 2) - 1
    return lax.rem(me + sign * away + count, count)


def ring_source(me, step, count):
    away = (step + 1) // 2
    sign = 2 * lax.rem(step, 2) - 1
    return lax.rem(me - sign * away + count, count)


def slots_of(routes, capacity, experts):
    tokens = routes.shape[1]
    expert = lax.broadcasted_iota(jnp.int32, (experts, tokens), 0)
    first = expert == routes[0:1, :]
    second = expert == routes[1:2, :]
    row = lax.broadcasted_iota(jnp.int32, (tokens, tokens), 0)
    column = lax.broadcasted_iota(jnp.int32, (tokens, tokens), 1)
    earlier = jnp.where(row < column, 1.0, 0.0).astype(BF16)
    ones = jnp.ones((tokens, tokens), BF16)
    first_hot = jnp.where(first, 1.0, 0.0).astype(BF16)
    second_hot = jnp.where(second, 1.0, 0.0).astype(BF16)
    first_rank = dot(first_hot, earlier)
    second_rank = dot(first_hot, ones) + dot(second_hot, earlier)
    places = []
    for hot, rank, route in ((first, first_rank, routes[0:1, :]), (second, second_rank, routes[1:2, :])):
        own = jnp.sum(jnp.where(hot, rank, 0.0), axis=0, keepdims=True)
        places.append(route * capacity + own.astype(jnp.int32))
    return places


class Ring:
    def __init__(self, ref, item, me, count, sends, arrivals):
        self.ref, self.item, self.me, self.count = ref, item, me, count
        self.sends, self.arrivals = sends, arrivals
        self.half = ref.shape[1] // 2

    def copy(self, kind):
        right = lax.rem(self.me + 1, self.count)
        left = lax.rem(self.me + self.count - 1, self.count)
        first, last = pl.ds(0, self.half), pl.ds(self.half, self.half)
        source, target = (
            (self.ref.at[self.me], right),
            (self.ref.at[self.me], left),
            (self.ref.at[left, first], right),
            (self.ref.at[right, last], left),
        )[kind]
        return pltpu.make_async_remote_copy(
            src_ref=source,
            dst_ref=source,
            send_sem=self.sends.at[self.item, kind],
            recv_sem=self.arrivals.at[self.item, kind],
            device_id={"tp": target},
            device_id_type=MESH,
        )

    def arrival(self, kind):
        right = lax.rem(self.me + 1, self.count)
        left = lax.rem(self.me + self.count - 1, self.count)
        across = lax.rem(self.me + 2, self.count)
        first, last = pl.ds(0, self.half), pl.ds(self.half, self.half)
        source, landed = (
            (self.ref.at[self.me], self.ref.at[left]),
            (self.ref.at[self.me], self.ref.at[right]),
            (self.ref.at[left, first], self.ref.at[across, first]),
            (self.ref.at[right, last], self.ref.at[across, last]),
        )[kind]
        return pltpu.make_async_remote_copy(
            src_ref=source,
            dst_ref=landed,
            send_sem=self.sends.at[self.item, kind],
            recv_sem=self.arrivals.at[self.item, kind],
            device_id={"tp": right},
            device_id_type=MESH,
        )

    def start(self):
        self.copy(0).start()
        self.copy(1).start()

    def forward(self):
        self.arrival(0).wait_recv()
        self.copy(2).start()
        self.arrival(1).wait_recv()
        self.copy(3).start()

    def complete(self):
        self.arrival(2).wait_recv()
        self.arrival(3).wait_recv()

    def sent(self):
        for kind in range(4):
            self.copy(kind).wait_send()


def layer_kernel(sp_count, tp_count, head_count, *refs):
    chunks = len(WIDTHS)
    starts = [sum(WIDTHS[:n]) for n in range(chunks)]
    listed = refs[len(refs) - 3 * chunks :]
    refs = refs[: len(refs) - 3 * chunks]
    back_refs, answer_refs = listed[:chunks], listed[chunks : 2 * chunks]
    down_refs = listed[2 * chunks :]
    (
        q_hbm,
        k_hbm,
        v_hbm,
        og_hbm,
        ig_hbm,
        fg_hbm,
        hgain_hbm,
        wo_hbm,
        res_hbm,
        ngain_hbm,
        routes_hbm,
        group_hbm,
        scores_hbm,
        gate_hbm,
        up_hbm,
        down_hbm,
        out_ref,
        q_ref,
        k_ref,
        v_ref,
        og_ref,
        ig_ref,
        fg_ref,
        hgain_ref,
        wo_ref,
        res_ref,
        ngain_ref,
        routes_ref,
        group_ref,
        scores_ref,
        gate_ref,
        up_ref,
        intra_ref,
        peak_ref,
        s1_ref,
        s1s_ref,
        r1_ref,
        r1s_ref,
        s2_ref,
        s2s_ref,
        r2_ref,
        r2s_ref,
        s3_ref,
        r3_ref,
        mix_ref,
        mrecv_ref,
        stream_ref,
        send_ref,
        arrived_ref,
        hidden_ref,
        load_sem,
        send1,
        recv1,
        send1s,
        recv1s,
        send2,
        recv2,
        send2s,
        recv2s,
        send3,
        recv3,
        send4,
        recv4,
        send5,
        recv5,
        send6,
        recv6,
        ring_send,
        ring_recv,
    ) = refs
    me = lax.axis_index("sp")
    mt = lax.axis_index("tp")
    zed = me // PLANE
    place = lax.rem(me, PLANE)
    planes = sp_count // PLANE
    length, width = q_ref.shape
    head = width // head_count
    tokens = length // tp_count
    capacity = send_ref.shape[1]
    model = send_ref.shape[2]
    slots = sp_count * capacity

    barrier = pltpu.get_barrier_semaphore()

    loads = [
        (fg_hbm, fg_ref),
        (ig_hbm, ig_ref),
        (k_hbm, k_ref),
        (v_hbm, v_ref),
        (q_hbm, q_ref),
        (gate_hbm.at[0], gate_ref.at[mt]),
        (og_hbm, og_ref),
        (hgain_hbm, hgain_ref),
        (ngain_hbm, ngain_ref),
        (routes_hbm, routes_ref),
        (group_hbm, group_ref),
        (scores_hbm, scores_ref),
        (res_hbm, res_ref),
        (up_hbm.at[0], up_ref.at[mt]),
        (wo_hbm, wo_ref),
    ]
    for start, size, ref in zip(starts, WIDTHS, down_refs):
        loads.append((down_hbm.at[0, :, pl.ds(start, size)], ref.at[mt]))
    loads = [
        pltpu.make_async_copy(source, target, load_sem.at[n])
        for n, (source, target) in enumerate(loads)
    ]
    for load in loads[:6]:
        load.start()

    for step in range(1, PLANE):
        peer = zed * PLANE + lax.rem(place + step, PLANE)
        pl.semaphore_signal(barrier, inc=1, device_id={"sp": peer}, device_id_type=MESH)
    for step in range(1, planes):
        peer = lax.rem(zed + step, planes) * PLANE + place
        pl.semaphore_signal(barrier, inc=1, device_id={"sp": peer}, device_id_type=MESH)
    for step in range(1, tp_count):
        peer = lax.rem(mt + step, tp_count)
        pl.semaphore_signal(barrier, inc=1, device_id={"tp": peer}, device_id_type=MESH)

    early = 3 * model // 4
    gate_first = gate_ref.at[:, pl.ds(0, early), :]
    gate_last = gate_ref.at[:, pl.ds(early, model - early), :]
    gate_ring, gate_rest, up_ring, *down_rings = [
        Ring(ref, item, mt, tp_count, ring_send, ring_recv)
        for item, ref in enumerate((gate_first, gate_last, up_ref, *down_refs))
    ]
    for load in loads[:5]:
        load.wait()

    small = jnp.exp(-fg_ref[...])
    series = small * (1.0 - small * (0.5 - small * (1.0 / 3.0 - 0.25 * small)))
    log_forget = -jnp.where(small < 0.01, series, jnp.log(1.0 + small))
    cum = running(log_forget, jnp.add, 0.0)
    level_in = ig_ref[...] - cum
    peak = running(level_in, jnp.maximum, VERY_NEGATIVE)
    total_col = cum[:, length - 1 : length]
    top_col = peak[:, length - 1 : length]
    weight = jnp.exp(level_in - top_col)

    lane_head = lax.broadcasted_iota(jnp.int32, (1, width), 1) // head
    masks = [lane_head == h for h in range(head_count)]

    def spread(column):
        row = jnp.zeros((1, width), F32)
        for h in range(head_count):
            row = jnp.where(masks[h], column[h : h + 1, :], row)
        return row

    total_row = spread(total_col)
    level_row = total_row + spread(top_col)

    k_turned = k_ref[...].astype(F32).T
    parts = [
        k_turned[h * head : (h + 1) * head, :] * weight[h : h + 1, :] for h in range(head_count)
    ]
    high, low = halves(jnp.concatenate(parts, axis=0))
    values = v_ref[...]
    whole = dot(high, values) + dot(low, values)
    memory = jnp.zeros((head, width), F32)
    for h in range(head_count):
        memory = jnp.where(masks[h], whole[h * head : (h + 1) * head, :], memory)
    rows = head // PLANE
    for n in range(PLANE):
        s1_ref[n] = memory[n * rows : (n + 1) * rows, :]
    s1s_ref[0, 0:1, :] = total_row
    s1s_ref[0, 1:2, :] = level_row
    r1_ref[place] = s1_ref[place]
    r1s_ref[place] = s1s_ref[0]

    pl.semaphore_wait(barrier, PLANE + planes + tp_count - 3)
    loads[5].wait()

    def whole(source, landed, send_sem, recv_sem):
        return pltpu.make_async_remote_copy(
            src_ref=source,
            dst_ref=landed,
            send_sem=send_sem,
            recv_sem=recv_sem,
            device_id={"tp": lax.rem(mt + 1, tp_count)},
            device_id_type=MESH,
        )

    def exchange1(step):
        peer = lax.rem(place + step, PLANE)
        return pltpu.make_async_remote_copy(
            src_ref=s1_ref.at[peer],
            dst_ref=r1_ref.at[place],
            send_sem=send1,
            recv_sem=recv1,
            device_id={"sp": zed * PLANE + peer},
            device_id_type=MESH,
        )

    def exchange1s(step):
        peer = lax.rem(place + step, PLANE)
        return pltpu.make_async_remote_copy(
            src_ref=s1s_ref.at[0],
            dst_ref=r1s_ref.at[place],
            send_sem=send1s,
            recv_sem=recv1s,
            device_id={"sp": zed * PLANE + peer},
            device_id_type=MESH,
        )

    def exchange2s(step):
        peer = lax.rem(zed + step, planes)
        return pltpu.make_async_remote_copy(
            src_ref=s2s_ref.at[0],
            dst_ref=r2s_ref.at[zed],
            send_sem=send2s,
            recv_sem=recv2s,
            device_id={"sp": peer * PLANE + place},
            device_id_type=MESH,
        )

    def exchange2(step):
        peer = lax.rem(zed + step, planes)
        return pltpu.make_async_remote_copy(
            src_ref=s2_ref.at[0],
            dst_ref=r2_ref.at[zed],
            send_sem=send2,
            recv_sem=recv2,
            device_id={"sp": peer * PLANE + place},
            device_id_type=MESH,
        )

    def exchange3(step):
        peer = lax.rem(place + step, PLANE)
        return pltpu.make_async_remote_copy(
            src_ref=s3_ref.at[peer],
            dst_ref=r3_ref.at[place],
            send_sem=send3,
            recv_sem=recv3,
            device_id={"sp": zed * PLANE + peer},
            device_id_type=MESH,
        )

    rest = pl.ds(0, PLANE - 1)
    rest_planes = pl.ds(0, planes - 1)
    for step in range(1, PLANE):
        exchange1s(step).start()
        exchange1(step).start()
    gate_ring.start()
    for load in loads[6:]:
        load.start()

    peak_cols = jnp.concatenate([peak, jnp.zeros((8 - head_count, length), F32)], axis=0).T
    peak_wide = jnp.zeros((length, width), F32)
    for h in range(head_count):
        peak_wide = jnp.where(masks[h], peak_cols[:, h : h + 1], peak_wide)
    peak_ref[...] = peak_wide
    scale = head**-0.5
    block = 128

    def inner(t):
        span = (t + 1) * block
        rows_t = slice(t * block, span)
        query = q_ref[rows_t, :].astype(F32) * scale
        position = lax.broadcasted_iota(jnp.int32, (block, span), 0) + t * block
        source = lax.broadcasted_iota(jnp.int32, (block, span), 1)
        causal = source <= position
        found = jnp.zeros((block, width), F32)
        for h in range(head_count):
            mine = jnp.where(masks[h], query, 0.0).astype(BF16)
            scores = dot_t(mine, k_ref[0:span, :])
            gap = level_in[h : h + 1, 0:span] - peak_cols[rows_t, h : h + 1]
            pairs = scores * jnp.exp(jnp.where(causal, gap, VERY_NEGATIVE))
            pairs_high, pairs_low = halves(pairs)
            part = dot(pairs_high, v_ref[0:span, :]) + dot(pairs_low, v_ref[0:span, :])
            found = jnp.where(masks[h], part, found)
        intra_ref[rows_t, :] = found

    inner(0)
    inner(1)

    whole(r1s_ref.at[rest], r1s_ref.at[rest], send1s, recv1s).wait()
    whole(r1_ref.at[rest], r1_ref.at[rest], send1, recv1).wait()
    identity = (
        jnp.zeros((1, width), F32),
        jnp.full((1, width), VERY_NEGATIVE, F32),
        jnp.zeros((rows, width), F32),
    )
    prior = [identity]
    for n in range(PLANE):
        prior.append(join(prior[-1], unpacked(r1_ref, r1s_ref, n)))
    put(s2_ref, s2s_ref, 0, prior[-1])
    put(r2_ref, r2s_ref, zed, prior[-1])
    for step in range(1, planes):
        exchange2s(step).start()
        exchange2(step).start()

    inner(2)

    whole(r2s_ref.at[rest_planes], r2s_ref.at[rest_planes], send2s, recv2s).wait()
    whole(r2_ref.at[rest_planes], r2_ref.at[rest_planes], send2, recv2).wait()
    entering = identity
    for n in range(planes):
        later = join(entering, unpacked(r2_ref, r2s_ref, n))
        entering = tuple(jnp.where(n < zed, new, old) for new, old in zip(later, entering))
    prior_total, prior_level, _ = identity
    for n in range(PLANE):
        total, level, part = join(entering, prior[n])
        s3_ref[n] = part
        prior_total = jnp.where(place == n, total, prior_total)
        prior_level = jnp.where(place == n, level, prior_level)
    r3_ref[place] = s3_ref[place]
    for step in range(1, PLANE):
        exchange3(step).start()

    inner(3)

    whole(s3_ref.at[rest], r3_ref.at[rest], send3, recv3).wait()
    start_level = jnp.maximum(prior_level, prior_total)
    opening = jnp.exp(prior_level - start_level)
    began = jnp.concatenate([r3_ref[n] for n in range(PLANE)], axis=0) * opening
    blocks = jnp.concatenate([jnp.where(masks[h], began, 0.0) for h in range(head_count)], axis=0)
    block_high, block_low = halves(blocks)
    row_head = lax.broadcasted_iota(jnp.int32, (width, width), 0) // head
    column_head = lax.broadcasted_iota(jnp.int32, (width, width), 1) // head
    averaging = jnp.where(row_head == column_head, 1.0 / head, 0.0).astype(BF16)
    for load in loads[6:]:
        load.wait()
    gain = jnp.concatenate([hgain_ref[h : h + 1, :] for h in range(head_count)], axis=1)

    def exchange4(step):
        peer = lax.rem(mt + step, tp_count)
        return pltpu.make_async_remote_copy(
            src_ref=mix_ref.at[peer],
            dst_ref=mrecv_ref.at[mt],
            send_sem=send4,
            recv_sem=recv4,
            device_id={"tp": peer},
            device_id_type=MESH,
        )

    for step in (2, 1, 3, 0):
        peer = lax.rem(mt + step, tp_count)
        rows_t = pl.ds(pl.multiple_of(peer * tokens, tokens), tokens)
        queries = (q_ref[rows_t, :].astype(F32) * scale).astype(BF16)
        carried = dot(queries, block_high) + dot(queries, block_low)
        peak_wide = peak_ref[rows_t, :]
        level = jnp.maximum(peak_wide, start_level)
        cell = jnp.exp(peak_wide - level) * intra_ref[rows_t, :]
        cell = cell + jnp.exp(start_level - level) * carried
        square_high, square_low = halves(cell * cell)
        mean = dot(square_high, averaging) + dot(square_low, averaging)
        gate = 1.0 / (1.0 + jnp.exp(-og_ref[rows_t, :].astype(F32)))
        mixed = (gate * (cell * lax.rsqrt(mean + EPSILON) * gain)).astype(BF16)
        if step:
            mix_ref[peer] = mixed
            exchange4(step).start()
        else:
            mrecv_ref[mt] = mixed
    gate_rest.start()
    up_ring.start()

    routes = routes_ref[:, pl.ds(pl.multiple_of(mt * tokens, tokens), tokens)]
    first, second = slots_of(routes, capacity, sp_count)
    slot = lax.broadcasted_iota(jnp.int32, (slots, tokens), 0)
    select = jnp.where((slot == first) | (slot == second), 1.0, 0.0).astype(BF16)

    others = pl.ds(0, tp_count - 1)
    whole(mix_ref.at[others], mrecv_ref.at[others], send4, recv4).wait()
    gathered = jnp.concatenate([mrecv_ref[n] for n in range(tp_count)], axis=1)
    piece = 512
    squares = jnp.zeros((tokens, 1), F32)
    for n in range(model // piece):
        cols = slice(n * piece, (n + 1) * piece)
        projected = dot(gathered, wo_ref[:, cols])
        stream = (res_ref[:, cols].astype(F32) + projected).astype(BF16)
        stream_ref[:, cols] = stream
        stream = stream.astype(F32)
        squares = squares + jnp.sum(stream * stream, axis=1, keepdims=True)
    inverse = lax.rsqrt(squares * (1.0 / model) + EPSILON)
    for n in range(model // piece):
        cols = slice(n * piece, (n + 1) * piece)
        normed = (stream_ref[:, cols].astype(F32) * inverse * ngain_ref[:, cols]).astype(BF16)
        chosen = dot(select, normed).reshape(sp_count, capacity, piece)
        send_ref[:, :, cols] = chosen.astype(BF16)

    arrived_ref[0] = send_ref[me]
    row_parts = 2
    group = sp_count // row_parts

    def dispatch(step):
        peer = ring_peer(me, step, sp_count)
        return pltpu.make_async_remote_copy(
            src_ref=send_ref.at[peer],
            dst_ref=arrived_ref.at[step],
            send_sem=send5,
            recv_sem=recv5.at[step // group],
            device_id={"sp": peer},
            device_id_type=MESH,
        )

    def go(step, _):
        dispatch(step).start()
        return 0

    lax.fori_loop(1, sp_count, go, 0)
    gate_ring.forward()
    gate_rest.forward()
    down_rings[0].start()

    own = pl.ds(pl.multiple_of(mt * tokens, tokens), tokens)
    scores = scores_ref[:, own]
    most = jnp.maximum(scores[0:1, :], scores[1:2, :])
    first_exp = jnp.exp(scores[0:1, :] - most)
    second_exp = jnp.exp(scores[1:2, :] - most)
    share = group_ref[:, own] / (first_exp + second_exp)
    weights = jnp.where(slot == first, share * first_exp, 0.0)
    weights = jnp.where(slot == second, share * second_exp, weights).T
    weights_high, weights_low = halves(weights)

    up_ring.forward()

    many = slots // row_parts
    rows_in = arrived_ref.reshape(slots, model)

    def expert(part, quarter):
        rows_t = slice(part * many, (part + 1) * many)
        gated = dot(rows_in[rows_t, :], gate_ref[quarter])
        raised = dot(rows_in[rows_t, :], up_ref[quarter])
        hidden_ref[quarter, rows_t, :] = (gated / (1.0 + jnp.exp(-gated)) * raised).astype(BF16)

    for part in range(row_parts):
        landed = arrived_ref.at[pl.ds(part * group, group - (part == 0))]
        whole(landed, landed, send5, recv5.at[part]).wait_recv()

        def near(n, _):
            expert(part, lax.rem(mt + n + tp_count - 1, tp_count))
            return 0

        lax.fori_loop(0, 3, near, 0)
        if part == 0:
            down_rings[0].forward()
            down_rings[1].start()
    gate_ring.complete()
    gate_rest.complete()
    up_ring.complete()
    for part in range(row_parts):
        expert(part, lax.rem(mt + 2, tp_count))

    def give(chunk, step):
        peer = ring_source(me, step, sp_count)
        return pltpu.make_async_remote_copy(
            src_ref=back_refs[chunk].at[step],
            dst_ref=answer_refs[chunk].at[me],
            send_sem=send6.at[chunk],
            recv_sem=recv6.at[chunk],
            device_id={"sp": peer},
            device_id_type=MESH,
        )

    def answer(chunk):
        down_ref, back_ref = down_refs[chunk], back_refs[chunk]
        wide = 384 if WIDTHS[chunk] == 384 else 256
        for n in range(WIDTHS[chunk] // wide):
            cols = slice(n * wide, (n + 1) * wide)
            result = jnp.zeros((slots, wide), F32)
            for quarter in range(tp_count):
                result = result + dot(hidden_ref[quarter], down_ref[quarter, :, cols])
            back_ref[:, :, cols] = result.reshape(sp_count, capacity, wide).astype(BF16)
        answer_refs[chunk][me] = back_ref[0]

        def go(step, _):
            give(chunk, step).start()
            return 0

        lax.fori_loop(1, sp_count, go, 0)

    def finish(chunk):
        back, landed = back_refs[chunk], answer_refs[chunk]
        most_of = pl.ds(0, sp_count - 1)
        whole(back.at[most_of], landed.at[most_of], send6.at[chunk], recv6.at[chunk]).wait()
        answers = answer_refs[chunk].reshape(slots, WIDTHS[chunk])[...]
        mix = dot(weights_high, answers) + dot(weights_low, answers)
        cols = slice(starts[chunk], starts[chunk] + WIDTHS[chunk])
        out_ref[:, cols] = (stream_ref[:, cols].astype(F32) + mix).astype(BF16)

    for chunk in range(chunks):
        if chunk:
            down_rings[chunk].forward()
            if chunk + 1 < chunks:
                down_rings[chunk + 1].start()
        down_rings[chunk].complete()
        answer(chunk)
    for chunk in range(chunks):
        finish(chunk)
    left = send_ref.at[pl.ds(0, sp_count - 1)]
    whole(left, left, send5, recv5.at[0]).wait_send()
    for ring in (gate_ring, gate_rest, up_ring, *down_rings):
        ring.sent()


def shards(
    residual,
    queries,
    key_vectors,
    value_vectors,
    output_gate,
    input_gate,
    forget_gate,
    head_gain,
    output_weight,
    norm_gain,
    route_experts,
    group_weight,
    expert_scores,
    gate_weight,
    up_weight,
    down_weight,
):
    sp_count = lax.axis_size("sp")
    tp_count = lax.axis_size("tp")
    length, width = queries.shape
    head_count, head = input_gate.shape[1], head_gain.shape[1]
    tokens, model = residual.shape
    capacity = 4 * tokens // sp_count
    hidden_part = gate_weight.shape[2]
    planes = sp_count // PLANE
    slots = sp_count * capacity
    rows = head // PLANE
    dma = pltpu.SemaphoreType.DMA
    vmem = pltpu.VMEM
    return pl.pallas_call(
        functools.partial(layer_kernel, sp_count, tp_count, head_count),
        out_shape=jax.ShapeDtypeStruct((tokens, model), BF16),
        in_specs=[pl.BlockSpec(memory_space=pl.ANY)] * 16,
        out_specs=pl.BlockSpec(memory_space=pltpu.VMEM),
        scratch_shapes=[
            vmem((length, width), BF16),
            vmem((length, width), BF16),
            vmem((length, width), BF16),
            vmem((length, width), BF16),
            vmem((head_count, length), F32),
            vmem((head_count, length), F32),
            vmem((head_count, head), F32),
            vmem(output_weight.shape, BF16),
            vmem((tokens, model), BF16),
            vmem((1, model), F32),
            vmem((2, length), jnp.int32),
            vmem((1, length), F32),
            vmem((2, length), F32),
            vmem((tp_count, model, hidden_part), BF16),
            vmem((tp_count, model, hidden_part), BF16),
            vmem((length, width), F32),
            vmem((length, width), F32),
            vmem((PLANE, rows, width), F32),
            vmem((1, 2, width), F32),
            vmem((PLANE, rows, width), F32),
            vmem((PLANE, 2, width), F32),
            vmem((1, rows, width), F32),
            vmem((1, 2, width), F32),
            vmem((planes, rows, width), F32),
            vmem((planes, 2, width), F32),
            vmem((PLANE, rows, width), F32),
            vmem((PLANE, rows, width), F32),
            vmem((tp_count, tokens, width), BF16),
            vmem((tp_count, tokens, width), BF16),
            vmem((tokens, model), BF16),
            vmem((sp_count, capacity, model), BF16),
            vmem((sp_count, capacity, model), BF16),
            vmem((tp_count, slots, hidden_part), BF16),
            dma((15 + len(WIDTHS),)),
            dma,
            dma,
            dma,
            dma,
            dma,
            dma,
            dma,
            dma,
            dma,
            dma,
            dma,
            dma,
            dma,
            dma((2,)),
            dma((len(WIDTHS),)),
            dma((len(WIDTHS),)),
            dma((3 + len(WIDTHS), 4)),
            dma((3 + len(WIDTHS), 4)),
            *[vmem((sp_count, capacity, n), BF16) for n in WIDTHS],
            *[vmem((sp_count, capacity, n), BF16) for n in WIDTHS],
            *[vmem((tp_count, hidden_part, n), BF16) for n in WIDTHS],
        ],
        compiler_params=pltpu.CompilerParams(
            collective_id=0, has_side_effects=True, vmem_limit_bytes=66_000_000
        ),
    )(
        queries,
        key_vectors,
        value_vectors,
        output_gate,
        input_gate.T,
        forget_gate.T,
        head_gain,
        output_weight,
        residual,
        norm_gain.reshape(1, model),
        route_experts.T,
        group_weight.reshape(1, length),
        expert_scores.T,
        gate_weight,
        up_weight,
        down_weight,
    )


def solution(mesh):
    both = ("sp", "tp")
    return jax.shard_map(
        shards,
        mesh=mesh,
        in_specs=(
            P(both, None),
            P("sp", "tp"),
            P("sp", "tp"),
            P("sp", "tp"),
            P("sp", "tp"),
            P("sp", "tp"),
            P("sp", "tp"),
            P("tp", None),
            P(),
            P(),
            P("sp", None),
            P("sp"),
            P("sp", None),
            P("sp", None, "tp"),
            P("sp", None, "tp"),
            P("sp", "tp", None),
        ),
        out_specs=P(both, None),
        check_vma=False,
    )
```
